32 devices in a mesh: grp: 2 (over y), sp: 4 (over z), fs: 2 (over x), tp: 2 (over core).
Axes of the slice: x: 2, y: 2, z: 4, core: 2. Of those that a mesh axis runs over, the one named last changes fastest.
Arguments:
- tokens: bfloat16 [4, 2048, 2048], P(('grp', 'fs'), ('sp', 'tp')), parts along dimension 0, may hold values from -6 to 6
- norm_gain: float32 [2048], replicated, may hold values from 0.1 to 1.9
- w_bgate: bfloat16 [2048, 2048], P(('sp', 'fs'), 'tp'), may hold values from -0.125 to 0.125
- w_cgate: bfloat16 [2048, 2048], P(('sp', 'fs'), 'tp'), may hold values from -0.125 to 0.125
- w_conv_in: bfloat16 [2048, 2048], P(('sp', 'fs'), 'tp'), may hold values from -0.125 to 0.125
- conv_taps: bfloat16 [3, 2048], P(None, 'tp'), may hold values from -3.5 to 3.5
- w_query: bfloat16 [2048, 2048], P(('sp', 'fs'), 'tp'), may hold values from -0.13258252 to 0.13258252
- w_key: bfloat16 [2048, 256], P(('sp', 'fs'), 'tp'), may hold values from -4.02167 to 4.02167
- w_value: bfloat16 [2048, 256], P(('sp', 'fs'), 'tp'), may hold values from -0.125 to 0.125
- sink_logits: float32 [32], P('tp'), may hold values from 1 to 6
- conv_out_weight: bfloat16 [2048, 2048], P('tp', ('sp', 'fs')), may hold values from -0.125 to 0.125
- attn_out_weight: bfloat16 [2048, 2048], P('tp', ('sp', 'fs')), may hold values from -0.75 to 0.75
Outputs:
- mixed: bfloat16 [4, 2048, 2048], P(('grp', 'fs'), ('sp', 'tp')), parts along dimension 0
The draws below stay inside these ranges and needn't reach their ends.
There are 2 independent parts, one for each index of `grp`. The reference program is written for one: setup_inputs(seed, part) draws one part's arguments, and reference() takes and returns one part's arrays. A program takes and returns all parts, laid end to end along the dimension named above; an argument that names none is the same for every part. Nothing has to cross between parts.
All inputs are finite; a program needn't handle non-finite values.
Results may differ from the reference program's by a relative error of at most 0.014.
The reference program's roundings to bfloat16 on the way count: a program that leaves them out, or rounds other values in their place, can miss the bound.
Values may be sent and summed in bfloat16 or wider, within the bound.
A program may use at most 128 MiB of HBM per device.

```python
import jax
import jax.numpy as jnp
from jax import lax

D = 2048
CONV = 2048
HEADS = 32
KV_HEADS = 4
HEAD = 64
WINDOW = 128
TAPS = 3
ATTN_Q = 2048
ATTN_KV = 256
SEQS = 2
LENGTH = 2048
N_TP = 2


def query_matrix(key):
    raw = jax.random.normal(jax.random.fold_in(key, 31), (D, ATTN_Q), jnp.float32)
    return jnp.clip(raw, -6.0, 6.0) / jnp.sqrt(jnp.float32(D))


def draw_w_query(key, part):
    return query_matrix(key).astype(jnp.bfloat16)


def draw_w_key(key, part):
    raw = jax.random.normal(jax.random.fold_in(key, 32), (D, ATTN_KV), jnp.float32)
    noise = jnp.clip(raw, -6.0, 6.0) / jnp.sqrt(jnp.float32(D))
    return noise.astype(jnp.bfloat16)


def draw_tokens(key, part):
    base = jnp.clip(jax.random.normal(jax.random.fold_in(key, 41), (SEQS, LENGTH, D), jnp.float32), -6.0, 6.0)
    return base.astype(jnp.bfloat16)


def steps_of(rng, shape, shards, smallest, high):
    gain = 1.0
    for dim, parts in shards:
        draws = jax.random.uniform(jax.random.fold_in(jax.random.fold_in(rng, 6), dim), (parts,), jnp.float32, smallest / len(shards), high / len(shards))
        gain = gain * jnp.repeat(jnp.exp(draws), shape[dim] // parts).reshape((-1,) + (1,) * (len(shape) - 1 - dim))
    return gain


def normal_values(own_key, shape, spread, bound, pieces=(), kind=jnp.bfloat16):
    array = jax.random.normal(own_key, shape, jnp.float32) * spread
    if len(pieces) > 0:
        array = steps_of(own_key, shape, pieces, -0.22, 0.18) * array
    return jnp.clip(array, min=-bound, max=bound).astype(kind)


def setup_inputs(seed: int = 0, part: int = 0) -> dict:
    key_list = jax.random.split(jax.random.key(seed), 13)
    own_keys = jax.random.split(jax.random.fold_in(key_list[12], part), 13)
    return {
        "tokens": draw_tokens(jax.random.fold_in(jax.random.fold_in(key_list[12], part), 71), part),
        "norm_gain": jnp.clip(1.0 + 0.18 * jax.random.normal(key_list[1], (D,), jnp.float32), 0.1, 1.9),
        "w_bgate": normal_values(key_list[2], (D, CONV), D ** -0.5, 0.125, ((0, 8), (1, 2))),
        "w_cgate": normal_values(key_list[3], (D, CONV), D ** -0.5, 0.125, ((0, 8), (1, 2))),
        "w_conv_in": normal_values(key_list[4], (D, CONV), D ** -0.5, 0.125, ((0, 8), (1, 2))),
        "conv_taps": normal_values(key_list[5], (TAPS, CONV), TAPS ** -0.5, 3.5, ((1, 2),)),
        "w_query": draw_w_query(jax.random.fold_in(key_list[12], 71), part),
        "w_key": draw_w_key(jax.random.fold_in(key_list[12], 71), part),
        "w_value": normal_values(key_list[8], (D, ATTN_KV), D ** -0.5, 0.125, ((0, 8), (1, 2))),
        "sink_logits": jnp.clip(1.0 + 5.0 * jax.random.uniform(key_list[9], (HEADS,), jnp.float32) ** steps_of(key_list[9], (HEADS,), ((0, 2),), -0.2, 0.2), 1.0, 6.0),
        "conv_out_weight": normal_values(key_list[10], (CONV, D), CONV ** -0.5, 0.125, ((0, 2), (1, 8))),
        "attn_out_weight": normal_values(key_list[11], (ATTN_Q, D), (ATTN_Q // 32) ** -0.5, 0.75, ((0, 2), (1, 8))),
    }


epsilon = 1e-06

def window_attention(queries, key_rows, value_rows, sink_logits):
    length = queries.shape[0]
    blocks = length // WINDOW
    groups = HEADS // KV_HEADS
    query_blocks = queries.astype(jnp.float32).reshape(blocks, WINDOW, KV_HEADS, groups, HEAD)
    zero_rows = jnp.zeros((WINDOW, ATTN_KV), jnp.float32)
    key_all = jnp.concatenate([zero_rows, key_rows.astype(jnp.float32)], 0)
    value_all = jnp.concatenate([zero_rows, value_rows.astype(jnp.float32)], 0)
    key_band = jnp.concatenate([key_all[:length].reshape(blocks, WINDOW, KV_HEADS, HEAD), key_all[WINDOW:].reshape(blocks, WINDOW, KV_HEADS, HEAD)], 1)
    value_band = jnp.concatenate([value_all[:length].reshape(blocks, WINDOW, KV_HEADS, HEAD), value_all[WINDOW:].reshape(blocks, WINDOW, KV_HEADS, HEAD)], 1)
    scores = jnp.einsum('nqhgd,nkhd->nhgqk', query_blocks, key_band) / jnp.sqrt(jnp.float32(HEAD))
    block_ids = jnp.arange(blocks)[:, None, None]
    query_pos = block_ids * WINDOW + jnp.arange(WINDOW)[None, :, None]
    key_pos = (block_ids - 1) * WINDOW + jnp.arange(2 * WINDOW)[None, None, :]
    allowed = (key_pos >= 0) & (key_pos <= query_pos) & (query_pos - key_pos < WINDOW)
    scores = jnp.where(allowed[:, None, None], scores, -jnp.inf)
    sink_grid = sink_logits.astype(jnp.float32).reshape(1, KV_HEADS, groups, 1, 1)
    peak_score = jnp.maximum(lax.optimization_barrier(jnp.max(scores, axis=-1, keepdims=True)), sink_grid)
    weights = jnp.exp(scores - peak_score)
    denominator = lax.optimization_barrier(jnp.sum(weights, axis=-1, keepdims=True)) + jnp.exp(sink_grid - peak_score)
    probabilities = (weights / denominator).astype(jnp.bfloat16)
    attended = jnp.einsum('nhgqk,nkhd->nqhgd', probabilities.astype(jnp.float32), value_band)
    return attended.astype(jnp.bfloat16).reshape(length, ATTN_Q)

def one_sequence(tokens, norm_gain, w_bgate, w_cgate, w_conv_in, conv_taps, w_query, w_key, w_value, sink_logits, conv_out_weight, attn_out_weight):
    widened = tokens.astype(jnp.float32)
    normed = (widened * lax.rsqrt(lax.optimization_barrier(jnp.mean(widened * widened, axis=-1, keepdims=True)) + epsilon) * norm_gain).astype(jnp.bfloat16)

    def project(weight):
        return jnp.dot(normed, weight, preferred_element_type=jnp.float32).astype(jnp.bfloat16)
    out_gate = project(w_bgate)
    in_gate = project(w_cgate)
    conv_input = project(w_conv_in)
    queries = project(w_query)
    key_rows = project(w_key)
    value_rows = project(w_value)
    length = tokens.shape[0]
    gated = (in_gate.astype(jnp.float32) * conv_input.astype(jnp.float32)).astype(jnp.bfloat16)
    padded = jnp.concatenate([jnp.zeros((TAPS - 1, CONV), jnp.bfloat16), gated], 0)
    taps_wide = conv_taps.astype(jnp.float32)
    convolved = padded[0:length].astype(jnp.float32) * taps_wide[0]
    for which in range(1, TAPS):
        convolved = convolved + padded[which:which + length].astype(jnp.float32) * taps_wide[which]
    conv_branch = (out_gate.astype(jnp.float32) * convolved).astype(jnp.bfloat16)
    attended = window_attention(queries, key_rows, value_rows, sink_logits)
    conv_parts = conv_branch.reshape(length, N_TP, CONV // N_TP)
    attn_parts = attended.reshape(length, N_TP, ATTN_Q // N_TP)
    conv_weight_parts = conv_out_weight.reshape(N_TP, CONV // N_TP, D)
    attn_weight_parts = attn_out_weight.reshape(N_TP, ATTN_Q // N_TP, D)
    running = jnp.zeros((length, D), jnp.float32)
    for member in range(N_TP):
        partial_value = jnp.dot(conv_parts[:, member], conv_weight_parts[member], preferred_element_type=jnp.float32)
        partial_value = partial_value + jnp.dot(attn_parts[:, member], attn_weight_parts[member], preferred_element_type=jnp.float32)
        rounded = lax.optimization_barrier(partial_value.astype(jnp.bfloat16))
        running = running + rounded.astype(jnp.float32)
    return running.astype(jnp.bfloat16)

def reference(tokens, norm_gain, w_bgate, w_cgate, w_conv_in, conv_taps, w_query, w_key, w_value, sink_logits, conv_out_weight, attn_out_weight):
    results = []
    for sequence in range(SEQS):
        results.append(one_sequence(tokens[sequence], norm_gain, w_bgate, w_cgate, w_conv_in, conv_taps, w_query, w_key, w_value, sink_logits, conv_out_weight, attn_out_weight))
    return jnp.stack(results, 0)
```

```python
import functools

import jax
import jax.numpy as jnp
from jax import lax
from jax.experimental import pallas as pl
from jax.experimental.pallas import tpu as pltpu
from jax.sharding import PartitionSpec as P

HEAD = 64
WINDOW = 128
TAPS = 3
LANES = 128
HALO = 16
LEAD = 2
MESH = pl.DeviceIdType.MESH

epsilon = 1e-06


def kernel(
    G,
    n,
    m,
    A,
    U,
    tokens,
    gain,
    w_key,
    w_value,
    w_query,
    w_cgate,
    w_conv_in,
    w_bgate,
    conv_weight,
    attn_weight,
    taps,
    sink,
    out,
    kvp,
    kvw,
    wbig,
    w_out,
    rows,
    kv,
    query,
    gate,
    ca,
    precv,
    send1,
    recv1,
    send2,
    recv2,
    fill_sem,
    fillo_sem,
    trade_send,
    trade_recv,
    otrade_send,
    otrade_recv,
    z_send,
    z_recv,
    tx_send,
    ty_send,
    td_send,
    tok_recv,
    hk_send,
    hk_recv,
    hg_send,
    hg_recv,
    d_send,
    d_recv,
    s1_send,
    s1_recv,
    s2_send,
    s2_recv,
):
    big = (w_query, w_cgate, w_conv_in, w_bgate)
    outputs = (conv_weight, attn_weight)
    own, features = tokens.shape
    length = 2 * own
    depth, kvwide = w_key.shape
    width = w_query.shape[1]
    Q = m * G
    slim = width // Q
    heads = slim // HEAD
    per_kv = width // kvwide
    across = conv_weight.shape[1]
    wa = across // A
    gw = features // U
    hw = gw // 2
    ins = 5 * m
    slots = ins + m * A
    bf16 = jnp.bfloat16

    g, s = lax.axis_index("grp"), lax.axis_index("sp")
    f, c = lax.axis_index("fs"), lax.axis_index("tp")
    q = f * G + g

    def loop(low, high, body):
        def step(i, carry):
            body(i)
            return carry

        lax.fori_loop(low, high, step, 0)

    def remote(source, target, send, recv, where):
        return pltpu.make_async_remote_copy(
            source, target, send, recv, device_id=where, device_id_type=MESH
        )

    def to_fs(e):
        return {"fs": lax.rem(f + e, m)}

    def to_grp(y):
        return {"grp": lax.rem(g + y, G)}

    other_core = {"tp": 1 - c}

    def seq(e, y):
        return lax.rem(f + e, m) * G + lax.rem(g + y, G)

    def nth(k):
        return seq(k // G, k % G)

    def kv_head(quarter):
        return quarter * heads // per_kv

    def weights(j, source, chunk):
        return kvw.at[source, chunk] if j == 0 else wbig.at[j - 1, source, chunk]

    def mine_of(j, quarter):
        if j == 0:
            return kvp.at[:, pl.ds(pl.multiple_of(kv_head(quarter) * 2 * HEAD, LANES), 2 * HEAD)]
        return big[j - 1].at[:, pl.ds(pl.multiple_of(quarter * slim, LANES), slim)]

    def out_of(j, a, quarter):
        return outputs[j].at[
            pl.ds(pl.multiple_of(quarter * slim, LANES), slim), pl.ds(a * wa, wa)
        ]

    def fill(j):
        return pltpu.make_async_copy(mine_of(j, q), weights(j, s, f), fill_sem.at[j])

    def fillo(j, a):
        return pltpu.make_async_copy(
            out_of(j, a, q), w_out.at[s, f, a, pl.ds(j * slim, slim)], fillo_sem.at[j, a]
        )

    for h in range(kvwide // HEAD):
        at = pl.ds(h * 2 * HEAD, 2 * HEAD)
        pick = slice(h * HEAD, (h + 1) * HEAD)
        kvp[:, at] = jnp.concatenate([w_key[:, pick], w_value[:, pick]], axis=1)

    for j in range(1, 5):
        fill(j).start()
    for j in range(2):
        for a in range(A):
            fillo(j, a).start()

    barrier = pltpu.get_barrier_semaphore()

    def greet(where):
        pl.semaphore_signal(barrier, inc=1, device_id=where, device_id_type=MESH)

    loop(1, n, lambda d: greet({"sp": lax.rem(s + d, n)}))
    loop(1, m, lambda e: greet(to_fs(e)))
    loop(1, G, lambda y: greet(to_grp(y)))
    greet(other_core)
    fill(0).start()
    pl.semaphore_wait(barrier, n + m + G - 2)

    def trade(j, e):
        t = lax.rem(f + e, m)
        return remote(
            mine_of(j, t * G + g),
            weights(j, s, f),
            trade_send.at[j, e],
            trade_recv.at[j, f],
            {"fs": t},
        )

    def trade_arrival(j, t):
        piece = weights(j, s, t)
        return remote(piece, piece, trade_send.at[j, 0], trade_recv.at[j, t], to_fs(1))

    def otrade(j, a, e):
        t = lax.rem(f + e, m)
        return remote(
            out_of(j, a, t * G + g),
            w_out.at[s, f, a, pl.ds(j * slim, slim)],
            otrade_send.at[j, a, e],
            otrade_recv.at[j, a, f],
            {"fs": t},
        )

    def otrade_arrival(j, a, t):
        piece = w_out.at[s, t, a, pl.ds(j * slim, slim)]
        return remote(piece, piece, otrade_send.at[j, a, 0], otrade_recv.at[j, a, t], to_fs(1))

    def piece(k, source):
        if k < ins:
            return weights(k // m, source, lax.rem(f + k % m, m))
        h, a = (k - ins) // A, (k - ins) % A
        return w_out.at[source, h, a]

    def z_copy(k, source, up, there):
        block = piece(k, source)
        return remote(
            block, block, z_send.at[k, up, source], z_recv.at[k, source], {"sp": there}
        )

    above, below = jnp.minimum(s + 1, n - 1), jnp.maximum(s - 1, 0)

    def own_start(k):
        if k < ins:
            j, h = k // m, k % m
            if h == 0:
                fill(j).wait()
            else:
                trade_arrival(j, lax.rem(f + h, m)).wait_recv()
        else:
            h, a = (k - ins) // A, (k - ins) % A
            for j in range(2):

                @pl.when(f == h)
                def _():
                    fillo(j, a).wait()

                @pl.when(f != h)
                def _():
                    otrade_arrival(j, a, h).wait_recv()

        @pl.when(s < n - 1)
        def _():
            z_copy(k, s, 0, above).start()

        @pl.when(s > 0)
        def _():
            z_copy(k, s, 1, below).start()

    def arrive(k, d):
        low, high = jnp.maximum(s - d, 0), jnp.minimum(s + d, n - 1)

        @pl.when(s - d >= 0)
        def _():
            z_copy(k, low, 0, above).wait_recv()

            @pl.when(s < n - 1)
            def _():
                z_copy(k, low, 0, above).start()

        @pl.when(s + d <= n - 1)
        def _():
            z_copy(k, high, 1, below).wait_recv()

            @pl.when(s > 0)
            def _():
                z_copy(k, high, 1, below).start()

    def arrivals_sent(k):
        @pl.when(s < n - 1)
        def _():
            loop(0, s + 1, lambda source: z_copy(k, source, 0, above).wait_send())

        @pl.when(s > 0)
        def _():
            loop(s, n, lambda source: z_copy(k, source, 1, below).wait_send())

    def tok(i, send, where):
        block = rows.at[i, pl.ds(pl.multiple_of(c * own, LANES), own)]
        return remote(block, block, send, tok_recv.at[i, c], where)

    def tok_x(e, y):
        return tok(seq(0, y), tx_send.at[e, y], to_fs(e))

    def tok_y(e, y):
        return tok(seq(e, 0), ty_send.at[e, y], to_grp(y))

    def tok_d(i):
        return tok(i, td_send.at[i], other_core)

    def tok_here(i, half):
        block = rows.at[i, pl.ds(pl.multiple_of(half * own, LANES), own)]
        return remote(block, block, td_send.at[i], tok_recv.at[i, half], other_core)

    def normalize():
        scale = gain[...]
        step = 16

        def body(t):
            at = pl.multiple_of(t * step, step)
            wide = tokens[pl.ds(at, step), :].astype(jnp.float32)
            norm = lax.rsqrt(jnp.mean(wide * wide, axis=-1, keepdims=True) + epsilon)
            rows[q, pl.ds(pl.multiple_of(c * own + at, step), step), :] = (
                wide * norm * scale
            ).astype(bf16)

        loop(0, own // step, body)

    def tokens_first():
        @pl.when(c == 0)
        def _():
            for e in range(1, m):
                tok_x(e, 0).start()
            for y in range(1, G):
                tok_y(0, y).start()

        @pl.when(c == 1)
        def _():
            for y in range(1, G):
                tok_y(0, y).start()
            for e in range(1, m):
                tok_x(e, 0).start()

        tok_d(q).start()

    def tokens_relay():
        @pl.when(c == 0)
        def _():
            for e in range(1, m):
                i = seq(e, 0)
                tok_here(i, c).wait_recv()
                for y in range(1, G):
                    tok_y(e, y).start()
                tok_d(i).start()

        @pl.when(c == 1)
        def _():
            for y in range(1, G):
                i = seq(0, y)
                tok_here(i, c).wait_recv()
                for e in range(1, m):
                    tok_x(e, y).start()
                tok_d(i).start()

    def tokens_near():
        def here(i):
            tok_here(i, c).wait_recv()
            tok_d(i).start()

        @pl.when(c == 0)
        def _():
            for y in range(1, G):
                here(seq(0, y))

        @pl.when(c == 1)
        def _():
            for e in range(1, m):
                here(seq(e, 0))

    def tokens_ready(k):
        i = nth(k)

        @pl.when((k // G > 0) & (k % G > 0))
        def _():
            tok_here(i, c).wait_recv()
            tok_d(i).start()

        tok_here(i, 1 - c).wait_recv()

    def tokens_sent():
        @pl.when(c == 0)
        def _():
            for e in range(1, m):
                tok_x(e, 0).wait_send()
            for e in range(m):
                for y in range(1, G):
                    tok_y(e, y).wait_send()

        @pl.when(c == 1)
        def _():
            for y in range(1, G):
                tok_y(0, y).wait_send()
            for e in range(1, m):
                for y in range(G):
                    tok_x(e, y).wait_send()

        loop(0, Q, lambda i: tok_d(i).wait_send())

    def halo_kv(i):
        return remote(
            kv.at[i, pl.ds(length, WINDOW)],
            kv.at[i, pl.ds(0, WINDOW)],
            hk_send.at[i],
            hk_recv.at[i],
            {"sp": above},
        )

    def halo_gate(i):
        return remote(
            gate.at[i, pl.ds(length, HALO)],
            gate.at[i, pl.ds(0, HALO)],
            hg_send.at[i],
            hg_recv.at[i],
            {"sp": above},
        )

    def project(j, i):
        block = kvw[...] if j == 0 else wbig[j - 1]
        block = block.reshape(n * m * depth, block.shape[-1])
        return jnp.dot(rows[i], block, preferred_element_type=jnp.float32)

    def do_keys(i):
        kv[i, pl.ds(WINDOW, length), :] = project(0, i).astype(bf16)

        @pl.when(s < n - 1)
        def _():
            halo_kv(i).start()

    def do_query(i):
        query[i] = project(1, i).astype(bf16)

    def do_gate(i):
        gate[i, pl.ds(HALO, length), :] = project(2, i).astype(bf16)

    def do_gated(i):
        values = project(3, i).astype(bf16).astype(jnp.float32)
        here = pl.ds(HALO, length)
        gate[i, here, :] = (gate[i, here, :].astype(jnp.float32) * values).astype(bf16)

        @pl.when(s < n - 1)
        def _():
            halo_gate(i).start()

    def do_conv(i):
        @pl.when(s > 0)
        def _():
            halo_gate(i).wait_recv()

        outer = project(4, i).astype(bf16).astype(jnp.float32)
        gated = gate[i].astype(jnp.float32)
        there = pl.ds(pl.multiple_of(q * slim, LANES), slim)
        mixed = None
        for which in range(TAPS):
            tap = taps[pl.ds(which, 1), there].astype(jnp.float32)
            low = HALO - TAPS + 1 + which
            term = tap * gated[low : low + length]
            mixed = term if mixed is None else mixed + term
        ca[i, :, pl.ds(0, slim)] = (outer * mixed).astype(bf16)

    pairs = 2 * HEAD
    blocks = length // WINDOW
    place_q = lax.broadcasted_iota(jnp.int32, (WINDOW, 2 * WINDOW), 0)
    place_k = lax.broadcasted_iota(jnp.int32, (WINDOW, 2 * WINDOW), 1)
    banded = (place_k > place_q) & (place_k <= place_q + WINDOW)

    def do_attention(i, b):
        row = pl.multiple_of(b * WINDOW, WINDOW)
        band = kv[i, pl.ds(row, 2 * WINDOW), :]
        key, value = band[:, :HEAD], band[:, HEAD:]
        least = jnp.where((s == 0) & (b == 0), WINDOW, 0)
        allowed = banded & (place_k >= least)
        for p in range(heads // 2):
            at = p * pairs
            both = query[i, pl.ds(row, WINDOW), pl.ds(at, pairs)]
            results = []
            for half in range(2):
                one = both[:, half * HEAD : (half + 1) * HEAD]
                scores = lax.dot_general(
                    one, key, (((1,), (1,)), ((), ())), preferred_element_type=jnp.float32
                ) * (1.0 / HEAD**0.5)
                scores = jnp.where(allowed, scores, -jnp.inf)
                logit = sink[q * heads + 2 * p + half]
                peak = jnp.maximum(jnp.max(scores, axis=-1, keepdims=True), logit)
                powers = jnp.exp(scores - peak)
                norm = jnp.sum(powers, axis=-1, keepdims=True) + jnp.exp(logit - peak)
                probs = (powers / norm).astype(bf16)
                results.append(jnp.dot(probs, value, preferred_element_type=jnp.float32))
            ca[i, pl.ds(row, WINDOW), pl.ds(slim + at, pairs)] = jnp.concatenate(
                results, axis=1
            ).astype(bf16)

    def columns(u, v=0, count=gw):
        return pl.ds(u * gw + v * hw, count)

    def half_rows(half):
        return pl.ds(pl.multiple_of(half * own, LANES), own)

    def core_copy(u, i):
        return remote(
            rows.at[i, half_rows(1 - c), columns(u)],
            precv.at[u, i],
            d_send.at[u, i],
            d_recv.at[u, i],
            other_core,
        )

    def chunk_of(u, t):
        if U == 1:
            return w_out[t // m, t % m, 0]
        return w_out[t, u // A, u % A]

    def do_out(u, i):
        per = max(1, min(2 * LANES, gw) // wa)

        for t in range(gw // (per * wa)):
            block = jnp.concatenate([chunk_of(u, t * per + k) for k in range(per)], axis=1)
            rows[i, :, pl.ds(u * gw + t * per * wa, per * wa)] = jnp.dot(
                ca[i], block, preferred_element_type=jnp.float32
            ).astype(bf16)
        core_copy(u, i).start()

    counts = ((G, m), (m, G))

    def ordered(v, first, second):
        return seq(second, first) if v == 0 else seq(first, second)

    def to_first(v, e):
        return to_grp(e) if v == 0 else to_fs(e)

    def to_second(v, e):
        return to_fs(e) if v == 0 else to_grp(e)

    def first_copy(u, v, e):
        n2 = counts[v][1]
        which = pl.ds((e - 1) * n2, n2)
        return remote(
            send1.at[u, v, which],
            recv1.at[u, v, which],
            s1_send.at[u, v, e - 1],
            s1_recv.at[u, v, e - 1],
            to_first(v, e),
        )

    def second_copy(u, v, e):
        return remote(
            send2.at[u, v, e - 1],
            recv2.at[u, v, e - 1],
            s2_send.at[u, v, e - 1],
            s2_recv.at[u, v, e - 1],
            to_second(v, e),
        )

    def both_cores(u, v, i):
        here = rows[i, half_rows(c), columns(u, v, hw)].astype(jnp.float32)
        return here + precv[u, i, :, pl.ds(v * hw, hw)].astype(jnp.float32)

    def stage_one(u):
        loop(0, Q, lambda i: core_copy(u, i).wait_recv())
        for v in range(2):
            n1, n2 = counts[v]
            for e in range(1, n1):
                for i2 in range(n2):
                    send1[u, v, (e - 1) * n2 + i2] = both_cores(u, v, ordered(v, e, i2)).astype(bf16)
                first_copy(u, v, e).start()

    def with_first(u, v, i2):
        n1, n2 = counts[v]
        value = both_cores(u, v, ordered(v, 0, i2))
        for e in range(1, n1):
            value = value + recv1[u, v, (e - 1) * n2 + i2].astype(jnp.float32)
        return value

    def stage_two(u):
        for v in range(2):
            n1, n2 = counts[v]
            for e in range(1, n1):
                first_copy(u, v, e).wait_recv()
            for i2 in range(1, n2):
                send2[u, v, i2 - 1] = with_first(u, v, i2).astype(bf16)
                second_copy(u, v, i2).start()

    def stage_three(u):
        for v in range(2):
            value = with_first(u, v, 0)
            for i2 in range(1, counts[v][1]):
                second_copy(u, v, i2).wait_recv()
                value = value + recv2[u, v, i2 - 1].astype(jnp.float32)
            value = value.astype(bf16)
            if U == 1:
                out[:, pl.ds(v * hw, hw)] = value
            else:
                for k in range(hw // wa):
                    source = v * (hw // wa) + k
                    chunk = source * m + u // A
                    at = chunk * across + (u % A) * wa
                    out[:, pl.ds(at, wa)] = value[:, k * wa : (k + 1) * wa]

    for j in range(5):
        loop(1, m, lambda e: trade(j, e).start())
        if j == 0:
            own_start(0)
    for k in range(1, LEAD):
        own_start(k)
    normalize()
    tokens_first()
    for j in range(2):
        for a in range(A):
            loop(1, m, lambda e: otrade(j, a, e).start())

    @pl.when(s == 0)
    def _():
        kv[:, pl.ds(0, WINDOW), :] = jnp.zeros((Q, WINDOW, 2 * HEAD), bf16)
        gate[:, pl.ds(0, HALO), :] = jnp.zeros((Q, HALO, slim), bf16)

    def attend(h, r):
        unit = h * 2 * G + r
        k, low = unit // 2, (unit % 2) * (blocks // 2)
        i = nth(k)

        @pl.when((s > 0) & (unit % 2 == 0))
        def _():
            halo_kv(i).wait_recv()

        loop(0, blocks // 2, lambda b: do_attention(i, low + b))

    def task(k, r):
        if k == 3 * m - 1:
            tokens_ready(r)
            do_keys(nth(r))
            do_query(nth(r))
        elif 3 * m <= k < 4 * m:
            attend(k - 3 * m, r)
        elif k == 4 * m:
            do_gate(nth(r))
        elif k == 4 * m + 1:
            do_gated(nth(r))
        elif k == ins:
            do_conv(nth(r))
        elif U > 1 and k > ins:
            do_out(k - ins - 1, nth(r))

    busy = set([3 * m - 1] + list(range(3 * m, 4 * m + 2)) + list(range(ins, slots)))
    for k in range(slots):
        if k + LEAD < slots:
            own_start(k + LEAD)
        if k == ins + 1:
            tokens_sent()
        turns = (2 * G if 3 * m <= k < 4 * m else Q) if k in busy else n - 1
        each = -(-(n - 1) // turns)

        def body(r):
            for dd in range(each):
                d = r * each + dd + 1

                @pl.when(d < n)
                def _():
                    arrive(k, d)

            task(k, r)

        loop(0, turns, body)
        if k == 2 * m - 1:
            tokens_relay()
        if k == 3 * m - 2:
            tokens_near()
        if U > 1 and k > ins:
            u = k - ins - 1
            if u >= 2:
                stage_three(u - 2)
            if u >= 1:
                stage_two(u - 1)
            stage_one(u)
    loop(0, Q, lambda r: do_out(U - 1, nth(r)))
    if U > 1:
        stage_two(U - 2)
    stage_one(U - 1)
    if U > 2:
        stage_three(U - 3)
    if U > 1:
        stage_three(U - 2)
    stage_two(U - 1)
    stage_three(U - 1)

    for j in range(5):
        loop(1, m, lambda e: trade(j, e).wait_send())
    for j in range(2):
        for a in range(A):
            loop(1, m, lambda e: otrade(j, a, e).wait_send())
    for k in range(slots):
        arrivals_sent(k)

    @pl.when(s < n - 1)
    def _():
        loop(0, Q, lambda i: halo_kv(i).wait_send())
        loop(0, Q, lambda i: halo_gate(i).wait_send())

    for u in range(U):
        loop(0, Q, lambda i: core_copy(u, i).wait_send())
        for v in range(2):
            for e in range(1, counts[v][0]):
                first_copy(u, v, e).wait_send()
            for e in range(1, counts[v][1]):
                second_copy(u, v, e).wait_send()


def local(
    G,
    n,
    m,
    tokens,
    norm_gain,
    w_bgate,
    w_cgate,
    w_conv_in,
    conv_taps,
    w_query,
    w_key,
    w_value,
    sink_logits,
    conv_out_weight,
    attn_out_weight,
):
    own, features = tokens.shape[1:]
    length = 2 * own
    depth, kvwide = w_key.shape
    width = w_query.shape[1]
    across = conv_out_weight.shape[1]
    Q = m * G
    slim = width // Q
    A = 2 if across % (2 * LANES) == 0 else 1
    U = m * A if across % LANES == 0 else 1
    wa = across // A
    gw = features // U
    slots = 5 * m + m * A
    n1, n2 = max(m, G) - 1, max(m, G)
    cnt = max((G - 1) * m, (m - 1) * G)
    bf16 = jnp.bfloat16
    vmem = pl.BlockSpec(memory_space=pltpu.VMEM)
    dma = pltpu.SemaphoreType.DMA
    mixed = pl.pallas_call(
        functools.partial(kernel, G, n, m, A, U),
        out_shape=jax.ShapeDtypeStruct((own, features), bf16),
        in_specs=[vmem] * 11 + [pl.BlockSpec(memory_space=pltpu.SMEM)],
        out_specs=vmem,
        scratch_shapes=[
            pltpu.VMEM((depth, 2 * kvwide), bf16),
            pltpu.VMEM((n, m, depth, 2 * HEAD), bf16),
            pltpu.VMEM((4, n, m, depth, slim), bf16),
            pltpu.VMEM((n, m, A, 2 * slim, wa), bf16),
            pltpu.VMEM((Q, length, features), bf16),
            pltpu.VMEM((Q, WINDOW + length, 2 * HEAD), bf16),
            pltpu.VMEM((Q, length, slim), bf16),
            pltpu.VMEM((Q, HALO + length, slim), bf16),
            pltpu.VMEM((Q, length, 2 * slim), bf16),
            pltpu.VMEM((U, Q, own, gw), bf16),
            pltpu.VMEM((U, 2, cnt, own, gw // 2), bf16),
            pltpu.VMEM((U, 2, cnt, own, gw // 2), bf16),
            pltpu.VMEM((U, 2, n1, own, gw // 2), bf16),
            pltpu.VMEM((U, 2, n1, own, gw // 2), bf16),
            dma((5,)),
            dma((2, A)),
            dma((5, m)),
            dma((5, m)),
            dma((2, A, m)),
            dma((2, A, m)),
            dma((slots, 2, n)),
            dma((slots, n)),
            dma((m, G)),
            dma((m, G)),
            dma((Q,)),
            dma((Q, 2)),
            dma((Q,)),
            dma((Q,)),
            dma((Q,)),
            dma((Q,)),
            dma((U, Q)),
            dma((U, Q)),
            dma((U, 2, n1)),
            dma((U, 2, n1)),
            dma((U, 2, n1)),
            dma((U, 2, n1)),
        ],
        compiler_params=pltpu.CompilerParams(
            collective_id=0, has_side_effects=True, vmem_limit_bytes=67_000_000
        ),
    )(
        tokens[0],
        norm_gain[None],
        w_key,
        w_value,
        w_query,
        w_cgate,
        w_conv_in,
        w_bgate,
        conv_out_weight,
        attn_out_weight,
        conv_taps,
        sink_logits,
    )
    return mixed[None]


def solution(mesh):
    placed = (
        P(("grp", "fs"), ("sp", "tp"), None),
        P(),
        P(("sp", "fs"), "tp"),
        P(("sp", "fs"), "tp"),
        P(("sp", "fs"), "tp"),
        P(None, "tp"),
        P(("sp", "fs"), "tp"),
        P(("sp", "fs"), "tp"),
        P(("sp", "fs"), "tp"),
        P("tp"),
        P("tp", ("sp", "fs")),
        P("tp", ("sp", "fs")),
    )
    return jax.shard_map(
        functools.partial(local, mesh.shape["grp"], mesh.shape["sp"], mesh.shape["fs"]),
        mesh=mesh,
        in_specs=placed,
        out_specs=P(("grp", "fs"), ("sp", "tp"), None),
        check_vma=False,
    )
```

```python
import functools

import jax
import jax.numpy as jnp
from jax import lax
from jax.experimental import pallas as pl
from jax.experimental.pallas import tpu as pltpu
from jax.sharding import PartitionSpec as P

HEAD = 64
WINDOW = 128
TAPS = 3
LANES = 128
HALO = 16
LEAD = 6
MESH = pl.DeviceIdType.MESH

KEYS = (2, 7, 10, 14)
QUERY = (6, 8, 11, 15)
ATTEND = (7, 11, 15, 19)
GATE = (12, 13, 16, 17)
GATED = (18, 19, 20, 21)
RELAY = (4, 5, 8, 13)

epsilon = 1e-06


def kernel(
    G,
    n,
    m,
    A,
    U,
    tokens,
    gain,
    w_key,
    w_value,
    w_query,
    w_cgate,
    w_conv_in,
    w_bgate,
    conv_weight,
    attn_weight,
    taps,
    sink,
    out,
    kvp,
    kvw,
    wbig,
    w_out,
    rows,
    kv,
    query,
    gate,
    ca,
    precv,
    send1,
    recv1,
    send2,
    recv2,
    fill_sem,
    fillo_sem,
    trade_send,
    trade_recv,
    otrade_send,
    otrade_recv,
    z_send,
    z_recv,
    tx_send,
    ty_send,
    td_send,
    tok_recv,
    hk_send,
    hk_recv,
    hg_send,
    hg_recv,
    d_send,
    d_recv,
    s1_send,
    s1_recv,
    s2_send,
    s2_recv,
):
    big = (w_query, w_cgate, w_conv_in, w_bgate)
    outputs = (conv_weight, attn_weight)
    own, features = tokens.shape
    length = 2 * own
    depth, kvwide = w_key.shape
    width = w_query.shape[1]
    Q = m * G
    slim = width // Q
    heads = slim // HEAD
    per_kv = width // kvwide
    across = conv_weight.shape[1]
    wa = across // A
    hr = own // 2
    ins = 5 * m
    slots = ins + m * A
    bf16 = jnp.bfloat16

    g, s = lax.axis_index("grp"), lax.axis_index("sp")
    f, c = lax.axis_index("fs"), lax.axis_index("tp")
    q = f * G + g

    def loop(low, high, body):
        def step(i, carry):
            body(i)
            return carry

        lax.fori_loop(low, high, step, 0)

    def remote(source, target, send, recv, where):
        return pltpu.make_async_remote_copy(
            source, target, send, recv, device_id=where, device_id_type=MESH
        )

    def to_fs(e):
        return {"fs": lax.rem(f + e, m)}

    def to_grp(y):
        return {"grp": lax.rem(g + y, G)}

    other_core = {"tp": 1 - c}

    def seq(e, y):
        return lax.rem(f + e, m) * G + lax.rem(g + y, G)

    def nth(k):
        return seq(k // G, k % G)

    def kv_head(quarter):
        return quarter * heads // per_kv

    def weights(j, source, chunk):
        return kvw.at[source, chunk] if j == 0 else wbig.at[j - 1, source, chunk]

    def mine_of(j, quarter):
        if j == 0:
            return kvp.at[:, pl.ds(pl.multiple_of(kv_head(quarter) * 2 * HEAD, LANES), 2 * HEAD)]
        return big[j - 1].at[:, pl.ds(pl.multiple_of(quarter * slim, LANES), slim)]

    def out_of(j, a, quarter):
        return outputs[j].at[
            pl.ds(pl.multiple_of(quarter * slim, LANES), slim), pl.ds(a * wa, wa)
        ]

    def fill(j):
        return pltpu.make_async_copy(mine_of(j, q), weights(j, s, f), fill_sem.at[j])

    def fillo(j, a):
        return pltpu.make_async_copy(
            out_of(j, a, q), w_out.at[s, f, a, pl.ds(j * slim, slim)], fillo_sem.at[j, a]
        )

    for h in range(kvwide // HEAD):
        at = pl.ds(h * 2 * HEAD, 2 * HEAD)
        pick = slice(h * HEAD, (h + 1) * HEAD)
        kvp[:, at] = jnp.concatenate([w_key[:, pick], w_value[:, pick]], axis=1)

    for j in range(1, 5):
        fill(j).start()
    for j in range(2):
        for a in range(A):
            fillo(j, a).start()

    barrier = pltpu.get_barrier_semaphore()

    def greet(where):
        pl.semaphore_signal(barrier, inc=1, device_id=where, device_id_type=MESH)

    loop(1, n, lambda d: greet({"sp": lax.rem(s + d, n)}))
    loop(1, m, lambda e: greet(to_fs(e)))
    loop(1, G, lambda y: greet(to_grp(y)))
    greet(other_core)
    fill(0).start()
    pl.semaphore_wait(barrier, n + m + G - 2)

    def trade(j, e):
        t = lax.rem(f + e, m)
        return remote(
            mine_of(j, t * G + g),
            weights(j, s, f),
            trade_send.at[j, e],
            trade_recv.at[j, f],
            {"fs": t},
        )

    def trade_arrival(j, t):
        piece = weights(j, s, t)
        return remote(piece, piece, trade_send.at[j, 0], trade_recv.at[j, t], to_fs(1))

    def otrade(j, a, e):
        t = lax.rem(f + e, m)
        return remote(
            out_of(j, a, t * G + g),
            w_out.at[s, f, a, pl.ds(j * slim, slim)],
            otrade_send.at[j, a, e],
            otrade_recv.at[j, a, f],
            {"fs": t},
        )

    def otrade_arrival(j, a, t):
        piece = w_out.at[s, t, a, pl.ds(j * slim, slim)]
        return remote(piece, piece, otrade_send.at[j, a, 0], otrade_recv.at[j, a, t], to_fs(1))

    def piece(k, source):
        if k < ins:
            return weights(k // m, source, lax.rem(f + k % m, m))
        h, a = (k - ins) // A, (k - ins) % A
        return w_out.at[source, h, a]

    def z_copy(k, source, up, there):
        block = piece(k, source)
        return remote(
            block, block, z_send.at[k, up, source], z_recv.at[k, source], {"sp": there}
        )

    above, below = jnp.minimum(s + 1, n - 1), jnp.maximum(s - 1, 0)

    def own_start(k):
        if k < ins:
            j, h = k // m, k % m
            if h == 0:
                fill(j).wait()
            else:
                trade_arrival(j, lax.rem(f + h, m)).wait_recv()
        else:
            h, a = (k - ins) // A, (k - ins) % A
            for j in range(2):

                @pl.when(f == h)
                def _():
                    fillo(j, a).wait()

                @pl.when(f != h)
                def _():
                    otrade_arrival(j, a, h).wait_recv()

        @pl.when(s < n - 1)
        def _():
            z_copy(k, s, 0, above).start()

        @pl.when(s > 0)
        def _():
            z_copy(k, s, 1, below).start()

    def arrive(k, d):
        low, high = jnp.maximum(s - d, 0), jnp.minimum(s + d, n - 1)

        @pl.when(s - d >= 0)
        def _():
            z_copy(k, low, 0, above).wait_recv()

            @pl.when(s < n - 1)
            def _():
                z_copy(k, low, 0, above).start()

        @pl.when(s + d <= n - 1)
        def _():
            z_copy(k, high, 1, below).wait_recv()

            @pl.when(s > 0)
            def _():
                z_copy(k, high, 1, below).start()

    def arrivals_sent(k):
        @pl.when(s < n - 1)
        def _():
            loop(0, s + 1, lambda source: z_copy(k, source, 0, above).wait_send())

        @pl.when(s > 0)
        def _():
            loop(s, n, lambda source: z_copy(k, source, 1, below).wait_send())

    def tok(i, send, where):
        block = rows.at[i, pl.ds(pl.multiple_of(c * own, LANES), own)]
        return remote(block, block, send, tok_recv.at[i, c], where)

    def tok_x(e, y):
        return tok(seq(0, y), tx_send.at[e, y], to_fs(e))

    def tok_y(e, y):
        return tok(seq(e, 0), ty_send.at[e, y], to_grp(y))

    def tok_d(i):
        return tok(i, td_send.at[i], other_core)

    def tok_here(i, half):
        block = rows.at[i, pl.ds(pl.multiple_of(half * own, LANES), own)]
        return remote(block, block, td_send.at[i], tok_recv.at[i, half], other_core)

    def normalize():
        scale = gain[...]
        step = 16

        def body(t):
            at = pl.multiple_of(t * step, step)
            wide = tokens[pl.ds(at, step), :].astype(jnp.float32)
            norm = lax.rsqrt(jnp.mean(wide * wide, axis=-1, keepdims=True) + epsilon)
            rows[q, pl.ds(pl.multiple_of(c * own + at, step), step), :] = (
                wide * norm * scale
            ).astype(bf16)

        loop(0, own // step, body)

    def tokens_first():
        @pl.when(c == 0)
        def _():
            for e in range(1, m):
                tok_x(e, 0).start()
            for y in range(1, G):
                tok_y(0, y).start()

        @pl.when(c == 1)
        def _():
            for y in range(1, G):
                tok_y(0, y).start()
            for e in range(1, m):
                tok_x(e, 0).start()

        tok_d(q).start()

    def tokens_relay(core):
        @pl.when(c == core)
        def _():
            for k in range(1, Q):
                e, y = k // G, k % G
                if core == 0 and y == 0:
                    tokens_on(nth(k))
                    for far in range(1, G):
                        tok_y(e, far).start()
                if core == 1 and e == 0:
                    tokens_on(nth(k))
                    for far in range(1, m):
                        tok_x(far, y).start()

    def tokens_on(i):
        tok_here(i, c).wait_recv()
        tok_d(i).start()

    def tokens_direct(core):
        @pl.when(c == core)
        def _():
            for k in range(1, Q):
                if (k // G == 0) == (core == 0) and (k // G) * (k % G) == 0:
                    tokens_on(nth(k))

    def tokens_far():
        for k in range(1, Q):
            if (k // G) * (k % G) > 0:
                tokens_on(nth(k))

    def tokens_sent():
        @pl.when(c == 0)
        def _():
            for e in range(1, m):
                tok_x(e, 0).wait_send()
            for e in range(m):
                for y in range(1, G):
                    tok_y(e, y).wait_send()

        @pl.when(c == 1)
        def _():
            for y in range(1, G):
                tok_y(0, y).wait_send()
            for e in range(1, m):
                for y in range(G):
                    tok_x(e, y).wait_send()

        loop(0, Q, lambda i: tok_d(i).wait_send())

    def halo_kv(i):
        return remote(
            kv.at[i, pl.ds(length, WINDOW)],
            kv.at[i, pl.ds(0, WINDOW)],
            hk_send.at[i],
            hk_recv.at[i],
            {"sp": above},
        )

    def halo_gate(i):
        return remote(
            gate.at[i, pl.ds(length, HALO)],
            gate.at[i, pl.ds(0, HALO)],
            hg_send.at[i],
            hg_recv.at[i],
            {"sp": above},
        )

    def project(j, i):
        block = kvw[...] if j == 0 else wbig[j - 1]
        block = block.reshape(n * m * depth, block.shape[-1])
        return jnp.dot(rows[i], block, preferred_element_type=jnp.float32)

    def do_keys(i):
        tok_here(i, 1 - c).wait_recv()
        kv[i, pl.ds(WINDOW, length), :] = project(0, i).astype(bf16)

        @pl.when(s < n - 1)
        def _():
            halo_kv(i).start()

    def do_query(i):
        query[i] = project(1, i).astype(bf16)

    def do_gate(i):
        gate[i, pl.ds(HALO, length), :] = project(2, i).astype(bf16)

    def do_gated(i):
        values = project(3, i).astype(bf16).astype(jnp.float32)
        here = pl.ds(HALO, length)
        gate[i, here, :] = (gate[i, here, :].astype(jnp.float32) * values).astype(bf16)

        @pl.when(s < n - 1)
        def _():
            halo_gate(i).start()

    def do_conv(i):
        @pl.when(s > 0)
        def _():
            halo_gate(i).wait_recv()

        outer = project(4, i).astype(bf16).astype(jnp.float32)
        gated = gate[i].astype(jnp.float32)
        there = pl.ds(pl.multiple_of(q * slim, LANES), slim)
        mixed = None
        for which in range(TAPS):
            tap = taps[pl.ds(which, 1), there].astype(jnp.float32)
            low = HALO - TAPS + 1 + which
            term = tap * gated[low : low + length]
            mixed = term if mixed is None else mixed + term
        ca[i, :, pl.ds(0, slim)] = (outer * mixed).astype(bf16)

    pairs = 2 * HEAD
    blocks = length // WINDOW
    place_q = lax.broadcasted_iota(jnp.int32, (WINDOW, 2 * WINDOW), 0)
    place_k = lax.broadcasted_iota(jnp.int32, (WINDOW, 2 * WINDOW), 1)
    banded = (place_k > place_q) & (place_k <= place_q + WINDOW)

    def do_attention(i, b):
        row = pl.multiple_of(b * WINDOW, WINDOW)
        band = kv[i, pl.ds(row, 2 * WINDOW), :]
        key, value = band[:, :HEAD], band[:, HEAD:]
        least = jnp.where((s == 0) & (b == 0), WINDOW, 0)
        allowed = banded & (place_k >= least)
        for p in range(heads // 2):
            at = p * pairs
            both = query[i, pl.ds(row, WINDOW), pl.ds(at, pairs)]
            results = []
            for half in range(2):
                one = both[:, half * HEAD : (half + 1) * HEAD]
                scores = lax.dot_general(
                    one, key, (((1,), (1,)), ((), ())), preferred_element_type=jnp.float32
                ) * (1.0 / HEAD**0.5)
                scores = jnp.where(allowed, scores, -jnp.inf)
                logit = sink[q * heads + 2 * p + half]
                peak = jnp.maximum(jnp.max(scores, axis=-1, keepdims=True), logit)
                powers = jnp.exp(scores - peak)
                norm = jnp.sum(powers, axis=-1, keepdims=True) + jnp.exp(logit - peak)
                probs = (powers / norm).astype(bf16)
                results.append(jnp.dot(probs, value, preferred_element_type=jnp.float32))
            ca[i, pl.ds(row, WINDOW), pl.ds(slim + at, pairs)] = jnp.concatenate(
                results, axis=1
            ).astype(bf16)

    def other_plane(d):
        return lax.rem(jnp.where(2 * s >= n, s - d + n, s + d), n)

    def chunks_of(u):
        if U == 1:
            return [(t // m, t % m, 0) for t in range(n * m)]
        if u == 0:
            return [(s, h, a) for h in range(m) for a in range(A)]
        return [(other_plane(d), (u - 1) // A, (u - 1) % A) for d in range(1, n)]

    lists = [chunks_of(u) for u in range(U)]
    sizes = [len(chunks) * wa for chunks in lists]
    firsts = [sum(sizes[:u]) for u in range(U)]

    def columns(u):
        return pl.ds(firsts[u], sizes[u])

    def half_rows(half):
        return pl.ds(pl.multiple_of(half * own, LANES), own)

    def core_copy(u, i):
        return remote(
            rows.at[i, half_rows(1 - c), columns(u)],
            precv.at[i, :, columns(u)],
            d_send.at[u, i],
            d_recv.at[u, i],
            other_core,
        )

    def do_out(u, i):
        per = max(1, 2 * LANES // wa)
        for t in range(0, len(lists[u]), per):
            some = lists[u][t : t + per]
            block = jnp.concatenate([w_out[p, h, a] for p, h, a in some], axis=1)
            rows[i, :, pl.ds(firsts[u] + t * wa, len(some) * wa)] = jnp.dot(
                ca[i], block, preferred_element_type=jnp.float32
            ).astype(bf16)
        core_copy(u, i).start()

    counts = ((G, m), (m, G))

    def ordered(v, first, second):
        return seq(second, first) if v == 0 else seq(first, second)

    def to_first(v, e):
        return to_grp(e) if v == 0 else to_fs(e)

    def to_second(v, e):
        return to_fs(e) if v == 0 else to_grp(e)

    def first_copy(u, v, e):
        n2 = counts[v][1]
        which = pl.ds((e - 1) * n2, n2)
        return remote(
            send1.at[v, which, :, columns(u)],
            recv1.at[v, which, :, columns(u)],
            s1_send.at[u, v, e - 1],
            s1_recv.at[u, v, e - 1],
            to_first(v, e),
        )

    def second_copy(u, v, e):
        return remote(
            send2.at[v, e - 1, :, columns(u)],
            recv2.at[v, e - 1, :, columns(u)],
            s2_send.at[u, v, e - 1],
            s2_recv.at[u, v, e - 1],
            to_second(v, e),
        )

    def both_cores(u, v, i):
        at = pl.ds(pl.multiple_of(c * own + v * hr, HALO), hr)
        here = rows[i, at, columns(u)].astype(jnp.float32)
        return here + precv[i, pl.ds(v * hr, hr), columns(u)].astype(jnp.float32)

    def stage_one(u):
        loop(0, Q, lambda i: core_copy(u, i).wait_recv())
        for v in range(2):
            n1, n2 = counts[v]
            for e in range(1, n1):
                for i2 in range(n2):
                    value = both_cores(u, v, ordered(v, e, i2))
                    send1[v, (e - 1) * n2 + i2, :, columns(u)] = value.astype(bf16)
                first_copy(u, v, e).start()

    def with_first(u, v, i2):
        n1, n2 = counts[v]
        value = both_cores(u, v, ordered(v, 0, i2))
        for e in range(1, n1):
            value = value + recv1[v, (e - 1) * n2 + i2, :, columns(u)].astype(jnp.float32)
        return value

    def stage_two(u):
        for v in range(2):
            n1, n2 = counts[v]
            for e in range(1, n1):
                first_copy(u, v, e).wait_recv()
            for i2 in range(1, n2):
                send2[v, i2 - 1, :, columns(u)] = with_first(u, v, i2).astype(bf16)
                second_copy(u, v, i2).start()

    def stage_three(u):
        for v in range(2):
            value = with_first(u, v, 0)
            for i2 in range(1, counts[v][1]):
                second_copy(u, v, i2).wait_recv()
                value = value + recv2[v, i2 - 1, :, columns(u)].astype(jnp.float32)
            value = value.astype(bf16)
            if U == 1:
                out[pl.ds(v * hr, hr), :] = value
            else:
                for k, (p, h, a) in enumerate(lists[u]):
                    at = pl.multiple_of((p * m + h) * across + a * wa, LANES)
                    out[pl.ds(v * hr, hr), pl.ds(at, wa)] = value[:, k * wa : (k + 1) * wa]

    for j in range(5):
        loop(1, m, lambda e: trade(j, e).start())
        if j == 0:
            own_start(0)
    for k in range(m, LEAD, m):
        own_start(k)
    normalize()
    tokens_first()
    for j in range(2):
        for a in range(A):
            loop(1, m, lambda e: otrade(j, a, e).start())
    for k in range(LEAD):
        if k % m > 0:
            own_start(k)

    @pl.when(s == 0)
    def _():
        kv[:, pl.ds(0, WINDOW), :] = jnp.zeros((Q, WINDOW, 2 * HEAD), bf16)
        gate[:, pl.ds(0, HALO), :] = jnp.zeros((Q, HALO, slim), bf16)

    def attend(unit):
        i = nth(unit // blocks)

        @pl.when((s > 0) & (unit % blocks == 0))
        def _():
            halo_kv(i).wait_recv()

        do_attention(i, unit % blocks)

    span = m * (n - 1)

    def place(base):
        return base * span // 6

    kinds = [0 if k == 0 else 1 if k // G == 0 else 2 if k % G == 0 else 3 for k in range(Q)]
    again = [kinds[:k].count(kinds[k]) for k in range(Q)]

    def times(bases):
        return [(place(bases[kinds[k]]) + again[k], k) for k in range(Q)]

    plan = [
        (do_keys, True, times(KEYS)),
        (do_query, True, times(QUERY)),
        (do_gate, True, times(GATE)),
        (do_gated, True, times(GATED)),
        (
            attend,
            False,
            [
                (place(ATTEND[kinds[k]] + b) + again[k], k * blocks + b)
                for k in range(Q)
                for b in range(blocks)
            ],
        ),
    ]
    relays = [
        (place(RELAY[0]), functools.partial(tokens_relay, 1)),
        (place(RELAY[1]), functools.partial(tokens_direct, 0)),
        (place(RELAY[2]), functools.partial(tokens_relay, 0)),
        (place(RELAY[2]), functools.partial(tokens_direct, 1)),
        (place(RELAY[3]), tokens_far),
    ]

    def tasks(first, count, r):
        for when, run in relays:
            if first <= when < first + count:
                pl.when(r == when - first)(run)
        for run, whole, entries in plan:
            here = [(t - first, k) for t, k in entries if first <= t < first + count]
            if here:
                hit, index = False, 0
                for t, k in here:
                    hit = (r == t) | hit
                    index = jnp.where(r == t, k, index)
                pl.when(hit)(functools.partial(run, nth(index) if whole else index))

    stages = {"o": lambda u: loop(0, Q, lambda r: do_out(u, nth(r)))}
    stages.update({"1": stage_one, "2": stage_two, "3": stage_three})
    events = {}
    last = U - 1
    if U > 1:
        for u in range(U):
            if u > 0:
                events.setdefault((ins + u - 1, n - 2), []).append(("o", u))
            for name, k, r in (("1", ins + u, 1 if u == 0 else 0), ("2", ins + u + 1, 1), ("3", ins + u + 2, 1)):
                if k < slots:
                    events.setdefault((k, min(r, n - 2)), []).append((name, u))

    for k in range(slots):
        if k + LEAD < slots:
            own_start(k + LEAD)
        if k == ins and U == 1:
            loop(0, Q, lambda r: do_conv(nth(r)))
            tokens_sent()
        if k >= ins and U > 1:
            for r in range(n - 1):
                if k == ins and r == 0:
                    loop(0, Q // 2, lambda i: do_conv(nth(i)))
                if k == ins and r == 1:
                    loop(Q // 2, Q, lambda i: do_conv(nth(i)))
                    tokens_sent()
                    stages["o"](0)
                arrive(k, r + 1)
                for name, u in sorted(events.get((k, r), []), key=lambda event: event[0]):
                    stages[name](u)
            continue

        def body(r):
            arrive(k, r + 1)
            if m <= k < ins:
                tasks((k - m) * (n - 1), n - 1, r)

        loop(0, n - 1, body)
    if U == 1:
        stages["o"](0)
    for name, u in (("1", last), ("2", last - 1), ("3", last - 2), ("3", last - 1), ("2", last), ("3", last)):
        if u >= 0:
            stages[name](u)

    for j in range(5):
        loop(1, m, lambda e: trade(j, e).wait_send())
    for j in range(2):
        for a in range(A):
            loop(1, m, lambda e: otrade(j, a, e).wait_send())
    for k in range(slots):
        arrivals_sent(k)

    @pl.when(s < n - 1)
    def _():
        loop(0, Q, lambda i: halo_kv(i).wait_send())
        loop(0, Q, lambda i: halo_gate(i).wait_send())

    for u in range(U):
        loop(0, Q, lambda i: core_copy(u, i).wait_send())
        for v in range(2):
            for e in range(1, counts[v][0]):
                first_copy(u, v, e).wait_send()
            for e in range(1, counts[v][1]):
                second_copy(u, v, e).wait_send()


def local(
    G,
    n,
    m,
    tokens,
    norm_gain,
    w_bgate,
    w_cgate,
    w_conv_in,
    conv_taps,
    w_query,
    w_key,
    w_value,
    sink_logits,
    conv_out_weight,
    attn_out_weight,
):
    own, features = tokens.shape[1:]
    length = 2 * own
    depth, kvwide = w_key.shape
    width = w_query.shape[1]
    across = conv_out_weight.shape[1]
    Q = m * G
    slim = width // Q
    A = 2 if across % (2 * LANES) == 0 else 1
    U = m * A + 1 if across % LANES == 0 else 1
    wa = across // A
    slots = 5 * m + m * A
    n1 = max(m, G) - 1
    cnt = max((G - 1) * m, (m - 1) * G)
    bf16 = jnp.bfloat16
    vmem = pl.BlockSpec(memory_space=pltpu.VMEM)
    dma = pltpu.SemaphoreType.DMA
    mixed = pl.pallas_call(
        functools.partial(kernel, G, n, m, A, U),
        out_shape=jax.ShapeDtypeStruct((own, features), bf16),
        in_specs=[vmem] * 11 + [pl.BlockSpec(memory_space=pltpu.SMEM)],
        out_specs=vmem,
        scratch_shapes=[
            pltpu.VMEM((depth, 2 * kvwide), bf16),
            pltpu.VMEM((n, m, depth, 2 * HEAD), bf16),
            pltpu.VMEM((4, n, m, depth, slim), bf16),
            pltpu.VMEM((n, m, A, 2 * slim, wa), bf16),
            pltpu.VMEM((Q, length, features), bf16),
            pltpu.VMEM((Q, WINDOW + length, 2 * HEAD), bf16),
            pltpu.VMEM((Q, length, slim), bf16),
            pltpu.VMEM((Q, HALO + length, slim), bf16),
            pltpu.VMEM((Q, length, 2 * slim), bf16),
            pltpu.VMEM((Q, own, features), bf16),
            pltpu.VMEM((2, cnt, own // 2, features), bf16),
            pltpu.VMEM((2, cnt, own // 2, features), bf16),
            pltpu.VMEM((2, n1, own // 2, features), bf16),
            pltpu.VMEM((2, n1, own // 2, features), bf16),
            dma((5,)),
            dma((2, A)),
            dma((5, m)),
            dma((5, m)),
            dma((2, A, m)),
            dma((2, A, m)),
            dma((slots, 2, n)),
            dma((slots, n)),
            dma((m, G)),
            dma((m, G)),
            dma((Q,)),
            dma((Q, 2)),
            dma((Q,)),
            dma((Q,)),
            dma((Q,)),
            dma((Q,)),
            dma((U, Q)),
            dma((U, Q)),
            dma((U, 2, n1)),
            dma((U, 2, n1)),
            dma((U, 2, n1)),
            dma((U, 2, n1)),
        ],
        compiler_params=pltpu.CompilerParams(
            collective_id=0, has_side_effects=True, vmem_limit_bytes=67_000_000
        ),
    )(
        tokens[0],
        norm_gain[None],
        w_key,
        w_value,
        w_query,
        w_cgate,
        w_conv_in,
        w_bgate,
        conv_out_weight,
        attn_out_weight,
        conv_taps,
        sink_logits,
    )
    return mixed[None]


def solution(mesh):
    placed = (
        P(("grp", "fs"), ("sp", "tp"), None),
        P(),
        P(("sp", "fs"), "tp"),
        P(("sp", "fs"), "tp"),
        P(("sp", "fs"), "tp"),
        P(None, "tp"),
        P(("sp", "fs"), "tp"),
        P(("sp", "fs"), "tp"),
        P(("sp", "fs"), "tp"),
        P("tp"),
        P("tp", ("sp", "fs")),
        P("tp", ("sp", "fs")),
    )
    return jax.shard_map(
        functools.partial(local, mesh.shape["grp"], mesh.shape["sp"], mesh.shape["fs"]),
        mesh=mesh,
        in_specs=placed,
        out_specs=P(("grp", "fs"), ("sp", "tp"), None),
        check_vma=False,
    )
```

```python
import functools

import jax
import jax.numpy as jnp
from jax import lax
from jax.experimental import pallas as pl
from jax.experimental.pallas import tpu as pltpu
from jax.sharding import PartitionSpec as P

HEAD = 64
WINDOW = 128
TAPS = 3
LANES = 128
HALO = 16
LEAD = 3
OUT_LEAD = 1
MESH = pl.DeviceIdType.MESH

KEYS = (2, 8, 11, 15)
QUERY = (6, 9, 12, 16)
ATTEND = (7, 11, 15, 19)
GATE = (12, 13, 14, 17)
GATED = (18, 19, 20, 21)
RELAY = (5, 6, 9, 14)

epsilon = 1e-06


def kernel(
    G,
    n,
    m,
    A,
    U,
    tokens,
    gain,
    w_key,
    w_value,
    w_query,
    w_cgate,
    w_conv_in,
    w_bgate,
    conv_weight,
    attn_weight,
    taps,
    sink,
    out,
    kvp,
    kvw,
    wbig,
    w_out,
    rows,
    kv,
    query,
    gate,
    ca,
    precv,
    send1,
    recv1,
    send2,
    recv2,
    fill_sem,
    fillo_sem,
    trade_send,
    trade_recv,
    otrade_send,
    otrade_recv,
    z_send,
    z_recv,
    tx_send,
    ty_send,
    td_send,
    tok_recv,
    hk_send,
    hk_recv,
    hg_send,
    hg_recv,
    d_send,
    d_recv,
    s1_send,
    s1_recv,
    s2_send,
    s2_recv,
):
    big = (w_query, w_cgate, w_conv_in, w_bgate)
    outputs = (conv_weight, attn_weight)
    own, features = tokens.shape
    length = 2 * own
    depth, kvwide = w_key.shape
    width = w_query.shape[1]
    Q = m * G
    slim = width // Q
    heads = slim // HEAD
    per_kv = width // kvwide
    across = conv_weight.shape[1]
    wa = across // A
    hr = own // 2
    ins = 5 * m
    slots = ins + m * A
    bf16 = jnp.bfloat16

    g, s = lax.axis_index("grp"), lax.axis_index("sp")
    f, c = lax.axis_index("fs"), lax.axis_index("tp")
    q = f * G + g

    def loop(low, high, body):
        def step(i, carry):
            body(i)
            return carry

        lax.fori_loop(low, high, step, 0)

    def remote(source, target, send, recv, where):
        return pltpu.make_async_remote_copy(
            source, target, send, recv, device_id=where, device_id_type=MESH
        )

    def to_fs(e):
        return {"fs": lax.rem(f + e, m)}

    def to_grp(y):
        return {"grp": lax.rem(g + y, G)}

    other_core = {"tp": 1 - c}

    def seq(e, y):
        return lax.rem(f + e, m) * G + lax.rem(g + y, G)

    def nth(k):
        return seq(k // G, k % G)

    def kv_head(quarter):
        return quarter * heads // per_kv

    def weights(j, source, chunk):
        return kvw.at[source, chunk] if j == 0 else wbig.at[j - 1, source, chunk]

    def mine_of(j, quarter):
        if j == 0:
            return kvp.at[:, pl.ds(pl.multiple_of(kv_head(quarter) * 2 * HEAD, LANES), 2 * HEAD)]
        return big[j - 1].at[:, pl.ds(pl.multiple_of(quarter * slim, LANES), slim)]

    def out_of(j, a, quarter):
        return outputs[j].at[
            pl.ds(pl.multiple_of(quarter * slim, LANES), slim), pl.ds(a * wa, wa)
        ]

    def fill(j):
        return pltpu.make_async_copy(mine_of(j, q), weights(j, s, f), fill_sem.at[j])

    def fillo(j, a):
        return pltpu.make_async_copy(
            out_of(j, a, q), w_out.at[s, f, a, pl.ds(j * slim, slim)], fillo_sem.at[j, a]
        )

    for h in range(kvwide // HEAD):
        at = pl.ds(h * 2 * HEAD, 2 * HEAD)
        pick = slice(h * HEAD, (h + 1) * HEAD)
        kvp[:, at] = jnp.concatenate([w_key[:, pick], w_value[:, pick]], axis=1)

    for j in range(1, 5):
        fill(j).start()
    for j in range(2):
        for a in range(A):
            fillo(j, a).start()

    barrier = pltpu.get_barrier_semaphore()

    def greet(where):
        pl.semaphore_signal(barrier, inc=1, device_id=where, device_id_type=MESH)

    loop(1, n, lambda d: greet({"sp": lax.rem(s + d, n)}))
    loop(1, m, lambda e: greet(to_fs(e)))
    loop(1, G, lambda y: greet(to_grp(y)))
    greet(other_core)
    fill(0).start()
    pl.semaphore_wait(barrier, n + m + G - 2)

    def trade(j, e):
        t = lax.rem(f + e, m)
        return remote(
            mine_of(j, t * G + g),
            weights(j, s, f),
            trade_send.at[j, e],
            trade_recv.at[j, f],
            {"fs": t},
        )

    def trade_arrival(j, t):
        piece = weights(j, s, t)
        return remote(piece, piece, trade_send.at[j, 0], trade_recv.at[j, t], to_fs(1))

    def otrade(j, a, e):
        t = lax.rem(f + e, m)
        return remote(
            out_of(j, a, t * G + g),
            w_out.at[s, f, a, pl.ds(j * slim, slim)],
            otrade_send.at[j, a, e],
            otrade_recv.at[j, a, f],
            {"fs": t},
        )

    def otrade_arrival(j, a, t):
        piece = w_out.at[s, t, a, pl.ds(j * slim, slim)]
        return remote(piece, piece, otrade_send.at[j, a, 0], otrade_recv.at[j, a, t], to_fs(1))

    def piece(k, source):
        if k < ins:
            return weights(k // m, source, lax.rem(f + k % m, m))
        h, a = (k - ins) // A, (k - ins) % A
        return w_out.at[source, h, a]

    def z_copy(k, source, up, there):
        block = piece(k, source)
        return remote(
            block, block, z_send.at[k, up, source], z_recv.at[k, source], {"sp": there}
        )

    above, below = jnp.minimum(s + 1, n - 1), jnp.maximum(s - 1, 0)

    ready = set()

    def own_ready(k):
        if k in ready:
            return
        ready.add(k)
        if k < ins:
            j, h = k // m, k % m
            if h == 0:
                fill(j).wait()
            else:
                trade_arrival(j, lax.rem(f + h, m)).wait_recv()
        else:
            h, a = (k - ins) // A, (k - ins) % A
            for j in range(2):

                @pl.when(f == h)
                def _():
                    fillo(j, a).wait()

                @pl.when(f != h)
                def _():
                    otrade_arrival(j, a, h).wait_recv()

    def own_start(k):
        own_ready(k)

        @pl.when(s < n - 1)
        def _():
            z_copy(k, s, 0, above).start()

        @pl.when(s > 0)
        def _():
            z_copy(k, s, 1, below).start()

    def arrive(k, d):
        low, high = jnp.maximum(s - d, 0), jnp.minimum(s + d, n - 1)

        @pl.when(s - d >= 0)
        def _():
            z_copy(k, low, 0, above).wait_recv()

            @pl.when(s < n - 1)
            def _():
                z_copy(k, low, 0, above).start()

        @pl.when(s + d <= n - 1)
        def _():
            z_copy(k, high, 1, below).wait_recv()

            @pl.when(s > 0)
            def _():
                z_copy(k, high, 1, below).start()

    def arrivals_sent(k):
        @pl.when(s < n - 1)
        def _():
            loop(0, s + 1, lambda source: z_copy(k, source, 0, above).wait_send())

        @pl.when(s > 0)
        def _():
            loop(s, n, lambda source: z_copy(k, source, 1, below).wait_send())

    def tok(i, send, where):
        block = rows.at[i, pl.ds(pl.multiple_of(c * own, LANES), own)]
        return remote(block, block, send, tok_recv.at[i, c], where)

    def tok_x(e, y):
        return tok(seq(0, y), tx_send.at[e, y], to_fs(e))

    def tok_y(e, y):
        return tok(seq(e, 0), ty_send.at[e, y], to_grp(y))

    def tok_d(i):
        return tok(i, td_send.at[i], other_core)

    def tok_here(i, half):
        block = rows.at[i, pl.ds(pl.multiple_of(half * own, LANES), own)]
        return remote(block, block, td_send.at[i], tok_recv.at[i, half], other_core)

    def normalize():
        scale = gain[...]
        step = 16

        def body(t):
            at = pl.multiple_of(t * step, step)
            wide = tokens[pl.ds(at, step), :].astype(jnp.float32)
            norm = lax.rsqrt(jnp.mean(wide * wide, axis=-1, keepdims=True) + epsilon)
            rows[q, pl.ds(pl.multiple_of(c * own + at, step), step), :] = (
                wide * norm * scale
            ).astype(bf16)

        loop(0, own // step, body)

    def tokens_first():
        @pl.when(c == 0)
        def _():
            for e in range(1, m):
                tok_x(e, 0).start()
            for y in range(1, G):
                tok_y(0, y).start()

        @pl.when(c == 1)
        def _():
            for y in range(1, G):
                tok_y(0, y).start()
            for e in range(1, m):
                tok_x(e, 0).start()

        tok_d(q).start()

    def tokens_relay(core):
        @pl.when(c == core)
        def _():
            for k in range(1, Q):
                e, y = k // G, k % G
                if core == 0 and y == 0:
                    tokens_on(nth(k))
                    for far in range(1, G):
                        tok_y(e, far).start()
                if core == 1 and e == 0:
                    tokens_on(nth(k))
                    for far in range(1, m):
                        tok_x(far, y).start()

    def tokens_on(i):
        tok_here(i, c).wait_recv()
        tok_d(i).start()

    def tokens_direct(core):
        @pl.when(c == core)
        def _():
            for k in range(1, Q):
                if (k // G == 0) == (core == 0) and (k // G) * (k % G) == 0:
                    tokens_on(nth(k))

    def tokens_far():
        for k in range(1, Q):
            if (k // G) * (k % G) > 0:
                tokens_on(nth(k))

    def trade_out():
        for j in range(2):
            for a in range(A):
                loop(1, m, lambda e: otrade(j, a, e).start())

    def tokens_sent():
        @pl.when(c == 0)
        def _():
            for e in range(1, m):
                tok_x(e, 0).wait_send()
            for e in range(m):
                for y in range(1, G):
                    tok_y(e, y).wait_send()

        @pl.when(c == 1)
        def _():
            for y in range(1, G):
                tok_y(0, y).wait_send()
            for e in range(1, m):
                for y in range(G):
                    tok_x(e, y).wait_send()

        loop(0, Q, lambda i: tok_d(i).wait_send())

    def halo_kv(i):
        return remote(
            kv.at[i, pl.ds(length, WINDOW)],
            kv.at[i, pl.ds(0, WINDOW)],
            hk_send.at[i],
            hk_recv.at[i],
            {"sp": above},
        )

    def halo_gate(i):
        return remote(
            gate.at[i, pl.ds(length, HALO)],
            gate.at[i, pl.ds(0, HALO)],
            hg_send.at[i],
            hg_recv.at[i],
            {"sp": above},
        )

    def project(j, i):
        block = kvw[...] if j == 0 else wbig[j - 1]
        block = block.reshape(n * m * depth, block.shape[-1])
        return jnp.dot(rows[i], block, preferred_element_type=jnp.float32)

    def do_keys(i):
        tok_here(i, 1 - c).wait_recv()
        kv[i, pl.ds(WINDOW, length), :] = project(0, i).astype(bf16)

        @pl.when(s < n - 1)
        def _():
            halo_kv(i).start()

    def do_query(i):
        query[i] = project(1, i).astype(bf16)

    def do_gate(i):
        gate[i, pl.ds(HALO, length), :] = project(2, i).astype(bf16)

    def do_gated(i):
        values = project(3, i).astype(bf16).astype(jnp.float32)
        here = pl.ds(HALO, length)
        gate[i, here, :] = (gate[i, here, :].astype(jnp.float32) * values).astype(bf16)

        @pl.when(s < n - 1)
        def _():
            halo_gate(i).start()

    def do_conv(i):
        @pl.when(s > 0)
        def _():
            halo_gate(i).wait_recv()

        outer = project(4, i).astype(bf16).astype(jnp.float32)
        gated = gate[i].astype(jnp.float32)
        there = pl.ds(pl.multiple_of(q * slim, LANES), slim)
        mixed = None
        for which in range(TAPS):
            tap = taps[pl.ds(which, 1), there].astype(jnp.float32)
            low = HALO - TAPS + 1 + which
            term = tap * gated[low : low + length]
            mixed = term if mixed is None else mixed + term
        ca[i, :, pl.ds(0, slim)] = (outer * mixed).astype(bf16)

    pairs = 2 * HEAD
    blocks = length // WINDOW
    place_q = lax.broadcasted_iota(jnp.int32, (WINDOW, 2 * WINDOW), 0)
    place_k = lax.broadcasted_iota(jnp.int32, (WINDOW, 2 * WINDOW), 1)
    banded = (place_k > place_q) & (place_k <= place_q + WINDOW)

    def do_attention(i, b):
        row = pl.multiple_of(b * WINDOW, WINDOW)
        band = kv[i, pl.ds(row, 2 * WINDOW), :]
        key, value = band[:, :HEAD], band[:, HEAD:]
        least = jnp.where((s == 0) & (b == 0), WINDOW, 0)
        allowed = banded & (place_k >= least)
        for p in range(heads // 2):
            at = p * pairs
            both = query[i, pl.ds(row, WINDOW), pl.ds(at, pairs)]
            results = []
            for half in range(2):
                one = both[:, half * HEAD : (half + 1) * HEAD]
                scores = lax.dot_general(
                    one, key, (((1,), (1,)), ((), ())), preferred_element_type=jnp.float32
                ) * (1.0 / HEAD**0.5)
                scores = jnp.where(allowed, scores, -jnp.inf)
                logit = sink[q * heads + 2 * p + half]
                peak = jnp.maximum(jnp.max(scores, axis=-1, keepdims=True), logit)
                powers = jnp.exp(scores - peak)
                norm = jnp.sum(powers, axis=-1, keepdims=True) + jnp.exp(logit - peak)
                probs = (powers / norm).astype(bf16)
                results.append(jnp.dot(probs, value, preferred_element_type=jnp.float32))
            ca[i, pl.ds(row, WINDOW), pl.ds(slim + at, pairs)] = jnp.concatenate(
                results, axis=1
            ).astype(bf16)

    def other_plane(d):
        return lax.rem(jnp.where(2 * s >= n, s - d + n, s + d), n)

    def chunks_of(u):
        if U == 1:
            return [(t // m, t % m, 0) for t in range(n * m)]
        if u == 0:
            return [(s, h, a) for h in range(m) for a in range(A)]
        k = min(u, m * A) - 1
        planes = range(1, n)
        if u == m * A:
            planes = range(1, n - 1)
        elif u > m * A:
            planes = range(n - 1, n)
        return [(other_plane(d), k // A, k % A) for d in planes]

    lists = [chunks_of(u) for u in range(U)]
    sizes = [len(chunks) * wa for chunks in lists]
    firsts = [sum(sizes[:u]) for u in range(U)]

    def columns(u):
        return pl.ds(firsts[u], sizes[u])

    def half_rows(half):
        return pl.ds(pl.multiple_of(half * own, LANES), own)

    def core_copy(u, i):
        return remote(
            rows.at[i, half_rows(1 - c), columns(u)],
            precv.at[i, :, columns(u)],
            d_send.at[u, i],
            d_recv.at[u, i],
            other_core,
        )

    def do_out(u, i):
        per = max(1, 2 * LANES // wa)
        for t in range(0, len(lists[u]), per):
            some = lists[u][t : t + per]
            block = jnp.concatenate([w_out[p, h, a] for p, h, a in some], axis=1)
            rows[i, :, pl.ds(firsts[u] + t * wa, len(some) * wa)] = jnp.dot(
                ca[i], block, preferred_element_type=jnp.float32
            ).astype(bf16)
        core_copy(u, i).start()

    counts = ((G, m), (m, G))

    def ordered(v, first, second):
        return seq(second, first) if v == 0 else seq(first, second)

    def to_first(v, e):
        return to_grp(e) if v == 0 else to_fs(e)

    def to_second(v, e):
        return to_fs(e) if v == 0 else to_grp(e)

    def first_copy(u, v, e):
        n2 = counts[v][1]
        which = pl.ds((e - 1) * n2, n2)
        return remote(
            send1.at[v, which, :, columns(u)],
            recv1.at[v, which, :, columns(u)],
            s1_send.at[u, v, e - 1],
            s1_recv.at[u, v, e - 1],
            to_first(v, e),
        )

    def second_copy(u, v, e):
        return remote(
            send2.at[v, e - 1, :, columns(u)],
            recv2.at[v, e - 1, :, columns(u)],
            s2_send.at[u, v, e - 1],
            s2_recv.at[u, v, e - 1],
            to_second(v, e),
        )

    def both_cores(u, v, i):
        at = pl.ds(pl.multiple_of(c * own + v * hr, HALO), hr)
        here = rows[i, at, columns(u)].astype(jnp.float32)
        return here + precv[i, pl.ds(v * hr, hr), columns(u)].astype(jnp.float32)

    def stage_one(u):
        loop(1, Q, lambda k: core_copy(u, nth(k)).wait_recv())
        for v in range(2):
            n1, n2 = counts[v]
            for e in range(1, n1):
                for i2 in range(n2):
                    value = both_cores(u, v, ordered(v, e, i2))
                    send1[v, (e - 1) * n2 + i2, :, columns(u)] = value.astype(bf16)
                first_copy(u, v, e).start()

    def with_first(u, v, i2):
        n1, n2 = counts[v]
        value = both_cores(u, v, ordered(v, 0, i2))
        for e in range(1, n1):
            value = value + recv1[v, (e - 1) * n2 + i2, :, columns(u)].astype(jnp.float32)
        return value

    def stage_two(u):
        for v in range(2):
            n1, n2 = counts[v]
            for e in range(1, n1):
                first_copy(u, v, e).wait_recv()
            for i2 in range(1, n2):
                send2[v, i2 - 1, :, columns(u)] = with_first(u, v, i2).astype(bf16)
                second_copy(u, v, i2).start()

    def stage_three(u):
        core_copy(u, q).wait_recv()
        for v in range(2):
            value = with_first(u, v, 0)
            for i2 in range(1, counts[v][1]):
                second_copy(u, v, i2).wait_recv()
                value = value + recv2[v, i2 - 1, :, columns(u)].astype(jnp.float32)
            value = value.astype(bf16)
            if U == 1:
                out[pl.ds(v * hr, hr), :] = value
            else:
                for k, (p, h, a) in enumerate(lists[u]):
                    at = pl.multiple_of((p * m + h) * across + a * wa, LANES)
                    out[pl.ds(v * hr, hr), pl.ds(at, wa)] = value[:, k * wa : (k + 1) * wa]

    for j in range(5):
        loop(1, m, lambda e: trade(j, e).start())
        if j == 0:
            own_start(0)
    for k in range(m, LEAD, m):
        own_start(k)
    normalize()
    tokens_first()
    for k in range(LEAD):
        if k % m > 0:
            own_start(k)

    @pl.when(s == 0)
    def _():
        kv[:, pl.ds(0, WINDOW), :] = jnp.zeros((Q, WINDOW, 2 * HEAD), bf16)
        gate[:, pl.ds(0, HALO), :] = jnp.zeros((Q, HALO, slim), bf16)

    def attend(unit):
        i = nth(unit // blocks)

        @pl.when((s > 0) & (unit % blocks == 0))
        def _():
            halo_kv(i).wait_recv()

        do_attention(i, unit % blocks)

    span = m * (n - 1)

    def place(base):
        return base * span // 6

    kinds = [0 if k == 0 else 1 if k // G == 0 else 2 if k % G == 0 else 3 for k in range(Q)]
    again = [kinds[:k].count(kinds[k]) for k in range(Q)]

    def times(bases):
        return [(place(bases[kinds[k]]) + again[k], k) for k in range(Q)]

    plan = [
        (do_keys, True, times(KEYS)),
        (do_query, True, times(QUERY)),
        (do_gate, True, times(GATE)),
        (do_gated, True, times(GATED)),
        (
            attend,
            False,
            [
                (place(ATTEND[kinds[k]] + b) + again[k], k * blocks + b)
                for k in range(Q)
                for b in range(blocks)
            ],
        ),
    ]
    relays = [
        (place(RELAY[0]), functools.partial(tokens_relay, 1)),
        (place(RELAY[1]), functools.partial(tokens_direct, 0)),
        (place(RELAY[2]), functools.partial(tokens_relay, 0)),
        (place(RELAY[2]), functools.partial(tokens_direct, 1)),
        (place(RELAY[3]), tokens_far),
        (place(RELAY[2] + 1), trade_out),
    ]

    def tasks(first, count, r):
        for when, run in relays:
            if first <= when < first + count:
                pl.when(r == when - first)(run)
        for run, whole, entries in plan:
            here = [(t - first, k) for t, k in entries if first <= t < first + count]
            if here:
                hit, index = False, 0
                for t, k in here:
                    hit = (r == t) | hit
                    index = jnp.where(r == t, k, index)
                pl.when(hit)(functools.partial(run, nth(index) if whole else index))

    stages = {"o": lambda u: loop(1, Q + 1, lambda r: do_out(u, nth(lax.rem(r, Q))))}
    stages.update({"1": stage_one, "2": stage_two, "3": stage_three})
    def finish(k):
        i = nth(lax.rem(k, Q))
        do_conv(i)
        do_out(0, i)

    last = U - 1
    after = {}
    for u in range(U - 2):
        k, low, high = ins + u, min(1, n - 2), n - 2
        if u > 0:
            after.setdefault((k, 0), []).append(("1", u))
        after.setdefault((k + 1, low), []).append(("2", u))
        after.setdefault((k + 2, low), []).append(("3", u))
        if u < U - 3:
            after.setdefault((k, high), []).append(("o", u + 1))
    ending = (
        [("2", last - 2), ("1", last), ("3", last - 3), ("2", last - 1)]
        + [("3", last - 2), ("2", last), ("3", last - 1), ("3", last)]
        if U > 1
        else [("1", 0), ("2", 0), ("3", 0)]
    )

    for k in range(slots):
        for later in range(LEAD, slots):
            if k == (later - LEAD if later < ins else max(later - OUT_LEAD, ins - LEAD)):
                own_start(later)
        if k == ins and U == 1:
            loop(0, Q, lambda r: do_conv(nth(r)))
            tokens_sent()
        if k >= ins and U > 1:
            for r in range(n - 1):
                if k == ins and r == 0:
                    for later in range(ins, slots):
                        own_ready(later)
                    tokens_sent()
                    loop(1, Q // 2 + 1, finish)
                if k == ins and r == 1:
                    loop(Q // 2 + 1, Q + 1, finish)
                    stages["1"](0)
                arrive(k, r + 1)
                if k == slots - 1 and r == n - 3:
                    stages["o"](last - 1)
                for name, u in after.get((k, r), []):
                    stages[name](u)
                if k == slots - 1 and r == n - 3:
                    stages["1"](last - 1)
                if k == slots - 1 and r == n - 2:
                    stages["o"](last)
            continue

        def body(r):
            arrive(k, r + 1)
            if m <= k < ins:
                tasks((k - m) * (n - 1), n - 1, r)

        loop(0, n - 1, body)
    if U == 1:
        stages["o"](0)
    for name, u in ending:
        stages[name](u)

    for j in range(5):
        loop(1, m, lambda e: trade(j, e).wait_send())
    for j in range(2):
        for a in range(A):
            loop(1, m, lambda e: otrade(j, a, e).wait_send())
    for k in range(slots):
        arrivals_sent(k)

    @pl.when(s < n - 1)
    def _():
        loop(0, Q, lambda i: halo_kv(i).wait_send())
        loop(0, Q, lambda i: halo_gate(i).wait_send())

    for u in range(U):
        loop(0, Q, lambda i: core_copy(u, i).wait_send())
        for v in range(2):
            for e in range(1, counts[v][0]):
                first_copy(u, v, e).wait_send()
            for e in range(1, counts[v][1]):
                second_copy(u, v, e).wait_send()


def local(
    G,
    n,
    m,
    tokens,
    norm_gain,
    w_bgate,
    w_cgate,
    w_conv_in,
    conv_taps,
    w_query,
    w_key,
    w_value,
    sink_logits,
    conv_out_weight,
    attn_out_weight,
):
    own, features = tokens.shape[1:]
    length = 2 * own
    depth, kvwide = w_key.shape
    width = w_query.shape[1]
    across = conv_out_weight.shape[1]
    Q = m * G
    slim = width // Q
    A = 2 if across % (2 * LANES) == 0 else 1
    U = m * A + 2 if across % LANES == 0 else 1
    wa = across // A
    slots = 5 * m + m * A
    n1 = max(m, G) - 1
    cnt = max((G - 1) * m, (m - 1) * G)
    bf16 = jnp.bfloat16
    vmem = pl.BlockSpec(memory_space=pltpu.VMEM)
    dma = pltpu.SemaphoreType.DMA
    mixed = pl.pallas_call(
        functools.partial(kernel, G, n, m, A, U),
        out_shape=jax.ShapeDtypeStruct((own, features), bf16),
        in_specs=[vmem] * 11 + [pl.BlockSpec(memory_space=pltpu.SMEM)],
        out_specs=vmem,
        scratch_shapes=[
            pltpu.VMEM((depth, 2 * kvwide), bf16),
            pltpu.VMEM((n, m, depth, 2 * HEAD), bf16),
            pltpu.VMEM((4, n, m, depth, slim), bf16),
            pltpu.VMEM((n, m, A, 2 * slim, wa), bf16),
            pltpu.VMEM((Q, length, features), bf16),
            pltpu.VMEM((Q, WINDOW + length, 2 * HEAD), bf16),
            pltpu.VMEM((Q, length, slim), bf16),
            pltpu.VMEM((Q, HALO + length, slim), bf16),
            pltpu.VMEM((Q, length, 2 * slim), bf16),
            pltpu.VMEM((Q, own, features), bf16),
            pltpu.VMEM((2, cnt, own // 2, features), bf16),
            pltpu.VMEM((2, cnt, own // 2, features), bf16),
            pltpu.VMEM((2, n1, own // 2, features), bf16),
            pltpu.VMEM((2, n1, own // 2, features), bf16),
            dma((5,)),
            dma((2, A)),
            dma((5, m)),
            dma((5, m)),
            dma((2, A, m)),
            dma((2, A, m)),
            dma((slots, 2, n)),
            dma((slots, n)),
            dma((m, G)),
            dma((m, G)),
            dma((Q,)),
            dma((Q, 2)),
            dma((Q,)),
            dma((Q,)),
            dma((Q,)),
            dma((Q,)),
            dma((U, Q)),
            dma((U, Q)),
            dma((U, 2, n1)),
            dma((U, 2, n1)),
            dma((U, 2, n1)),
            dma((U, 2, n1)),
        ],
        compiler_params=pltpu.CompilerParams(
            collective_id=0, has_side_effects=True, vmem_limit_bytes=67_000_000
        ),
    )(
        tokens[0],
        norm_gain[None],
        w_key,
        w_value,
        w_query,
        w_cgate,
        w_conv_in,
        w_bgate,
        conv_out_weight,
        attn_out_weight,
        conv_taps,
        sink_logits,
    )
    return mixed[None]


def solution(mesh):
    placed = (
        P(("grp", "fs"), ("sp", "tp"), None),
        P(),
        P(("sp", "fs"), "tp"),
        P(("sp", "fs"), "tp"),
        P(("sp", "fs"), "tp"),
        P(None, "tp"),
        P(("sp", "fs"), "tp"),
        P(("sp", "fs"), "tp"),
        P(("sp", "fs"), "tp"),
        P("tp"),
        P("tp", ("sp", "fs")),
        P("tp", ("sp", "fs")),
    )
    return jax.shard_map(
        functools.partial(local, mesh.shape["grp"], mesh.shape["sp"], mesh.shape["fs"]),
        mesh=mesh,
        in_specs=placed,
        out_specs=P(("grp", "fs"), ("sp", "tp"), None),
        check_vma=False,
    )
```

```python
import functools

import jax
import jax.numpy as jnp
from jax import lax
from jax.experimental import pallas as pl
from jax.experimental.pallas import tpu as pltpu
from jax.sharding import PartitionSpec as P

HEAD = 64
WINDOW = 128
TAPS = 3
LANES = 128
HALO = 16
LEAD = 3
OUT_LEAD = 1
MESH = pl.DeviceIdType.MESH

KEYS = (2, 8, 11, 15)
QUERY = (6, 9, 12, 16)
ATTEND = (7, 11, 15, 19)
GATE = (12, 13, 14, 17)
GATED = (18, 19, 20, 21)
RELAY = (5, 6, 9, 14)

epsilon = 1e-06


def kernel(
    G,
    n,
    m,
    A,
    U,
    tokens,
    gain,
    w_key,
    w_value,
    w_query,
    w_cgate,
    w_conv_in,
    w_bgate,
    conv_weight,
    attn_weight,
    taps,
    sink,
    out,
    kvp,
    kvw,
    wbig,
    w_out,
    rows,
    kv,
    query,
    gate,
    ca,
    precv,
    send1,
    recv1,
    send2,
    recv2,
    fill_sem,
    fillo_sem,
    trade_send,
    trade_recv,
    otrade_send,
    otrade_recv,
    z_send,
    z_recv,
    tx_send,
    ty_send,
    td_send,
    tok_recv,
    hk_send,
    hk_recv,
    hg_send,
    hg_recv,
    d_send,
    d_recv,
    s1_send,
    s1_recv,
    s2_send,
    s2_recv,
):
    big = (w_query, w_cgate, w_conv_in, w_bgate)
    outputs = (conv_weight, attn_weight)
    own, features = tokens.shape
    length = 2 * own
    depth, kvwide = w_key.shape
    width = w_query.shape[1]
    Q = m * G
    slim = width // Q
    heads = slim // HEAD
    per_kv = width // kvwide
    across = conv_weight.shape[1]
    wa = across // A
    hr = own // 2
    ins = 5 * m
    slots = ins + m * A
    bf16 = jnp.bfloat16

    g, s = lax.axis_index("grp"), lax.axis_index("sp")
    f, c = lax.axis_index("fs"), lax.axis_index("tp")
    q = f * G + g

    def loop(low, high, body):
        def step(i, carry):
            body(i)
            return carry

        lax.fori_loop(low, high, step, 0)

    def remote(source, target, send, recv, where):
        return pltpu.make_async_remote_copy(
            source, target, send, recv, device_id=where, device_id_type=MESH
        )

    def to_fs(e):
        return {"fs": lax.rem(f + e, m)}

    def to_grp(y):
        return {"grp": lax.rem(g + y, G)}

    other_core = {"tp": 1 - c}

    def seq(e, y):
        return lax.rem(f + e, m) * G + lax.rem(g + y, G)

    def nth(k):
        return seq(k // G, k % G)

    def kv_head(quarter):
        return quarter * heads // per_kv

    def weights(j, source, chunk):
        return kvw.at[source, chunk] if j == 0 else wbig.at[j - 1, source, chunk]

    def mine_of(j, quarter):
        if j == 0:
            return kvp.at[:, pl.ds(pl.multiple_of(kv_head(quarter) * 2 * HEAD, LANES), 2 * HEAD)]
        return big[j - 1].at[:, pl.ds(pl.multiple_of(quarter * slim, LANES), slim)]

    def out_of(j, a, quarter):
        return outputs[j].at[
            pl.ds(pl.multiple_of(quarter * slim, LANES), slim), pl.ds(a * wa, wa)
        ]

    def fill(j):
        return pltpu.make_async_copy(mine_of(j, q), weights(j, s, f), fill_sem.at[j])

    def fillo(j, a):
        return pltpu.make_async_copy(
            out_of(j, a, q), w_out.at[s, f, a, pl.ds(j * slim, slim)], fillo_sem.at[j, a]
        )

    for h in range(kvwide // HEAD):
        at = pl.ds(h * 2 * HEAD, 2 * HEAD)
        pick = slice(h * HEAD, (h + 1) * HEAD)
        kvp[:, at] = jnp.concatenate([w_key[:, pick], w_value[:, pick]], axis=1)

    for j in range(1, 5):
        fill(j).start()
    for j in range(2):
        for a in range(A):
            fillo(j, a).start()

    barrier = pltpu.get_barrier_semaphore()

    def greet(where):
        pl.semaphore_signal(barrier, inc=1, device_id=where, device_id_type=MESH)

    loop(1, n, lambda d: greet({"sp": lax.rem(s + d, n)}))
    loop(1, m, lambda e: greet(to_fs(e)))
    loop(1, G, lambda y: greet(to_grp(y)))
    greet(other_core)
    fill(0).start()
    pl.semaphore_wait(barrier, n + m + G - 2)

    def trade(j, e):
        t = lax.rem(f + e, m)
        return remote(
            mine_of(j, t * G + g),
            weights(j, s, f),
            trade_send.at[j, e],
            trade_recv.at[j, f],
            {"fs": t},
        )

    def trade_arrival(j, t):
        piece = weights(j, s, t)
        return remote(piece, piece, trade_send.at[j, 0], trade_recv.at[j, t], to_fs(1))

    def otrade(j, a, e):
        t = lax.rem(f + e, m)
        return remote(
            out_of(j, a, t * G + g),
            w_out.at[s, f, a, pl.ds(j * slim, slim)],
            otrade_send.at[j, a, e],
            otrade_recv.at[j, a, f],
            {"fs": t},
        )

    def otrade_arrival(j, a, t):
        piece = w_out.at[s, t, a, pl.ds(j * slim, slim)]
        return remote(piece, piece, otrade_send.at[j, a, 0], otrade_recv.at[j, a, t], to_fs(1))

    def piece(k, source):
        if k < ins:
            return weights(k // m, source, lax.rem(f + k % m, m))
        h, a = (k - ins) // A, (k - ins) % A
        return w_out.at[source, h, a]

    def z_copy(k, source, up, there):
        block = piece(k, source)
        return remote(
            block, block, z_send.at[k, up, source], z_recv.at[k, source], {"sp": there}
        )

    above, below = jnp.minimum(s + 1, n - 1), jnp.maximum(s - 1, 0)

    ready = set()

    def own_ready(k):
        if k in ready:
            return
        ready.add(k)
        if k < ins:
            j, h = k // m, k % m
            if h == 0:
                fill(j).wait()
            else:
                trade_arrival(j, lax.rem(f + h, m)).wait_recv()
        else:
            h, a = (k - ins) // A, (k - ins) % A
            for j in range(2):

                @pl.when(f == h)
                def _():
                    fillo(j, a).wait()

                @pl.when(f != h)
                def _():
                    otrade_arrival(j, a, h).wait_recv()

    def own_start(k):
        own_ready(k)

        @pl.when(s < n - 1)
        def _():
            z_copy(k, s, 0, above).start()

        @pl.when(s > 0)
        def _():
            z_copy(k, s, 1, below).start()

    def arrive(k, d):
        low, high = jnp.maximum(s - d, 0), jnp.minimum(s + d, n - 1)

        @pl.when(s - d >= 0)
        def _():
            z_copy(k, low, 0, above).wait_recv()

            @pl.when(s < n - 1)
            def _():
                z_copy(k, low, 0, above).start()

        @pl.when(s + d <= n - 1)
        def _():
            z_copy(k, high, 1, below).wait_recv()

            @pl.when(s > 0)
            def _():
                z_copy(k, high, 1, below).start()

    def arrivals_sent(k):
        @pl.when(s < n - 1)
        def _():
            loop(0, s + 1, lambda source: z_copy(k, source, 0, above).wait_send())

        @pl.when(s > 0)
        def _():
            loop(s, n, lambda source: z_copy(k, source, 1, below).wait_send())

    def tok(i, send, where):
        block = rows.at[i, pl.ds(pl.multiple_of(c * own, LANES), own)]
        return remote(block, block, send, tok_recv.at[i, c], where)

    def tok_x(e, y):
        return tok(seq(0, y), tx_send.at[e, y], to_fs(e))

    def tok_y(e, y):
        return tok(seq(e, 0), ty_send.at[e, y], to_grp(y))

    def tok_d(i):
        return tok(i, td_send.at[i], other_core)

    def tok_here(i, half):
        block = rows.at[i, pl.ds(pl.multiple_of(half * own, LANES), own)]
        return remote(block, block, td_send.at[i], tok_recv.at[i, half], other_core)

    def normalize():
        scale = gain[...]
        step = 16

        def body(t):
            at = pl.multiple_of(t * step, step)
            wide = tokens[pl.ds(at, step), :].astype(jnp.float32)
            norm = lax.rsqrt(jnp.mean(wide * wide, axis=-1, keepdims=True) + epsilon)
            rows[q, pl.ds(pl.multiple_of(c * own + at, step), step), :] = (
                wide * norm * scale
            ).astype(bf16)

        loop(0, own // step, body)

    def tokens_first():
        @pl.when(c == 0)
        def _():
            for e in range(1, m):
                tok_x(e, 0).start()
            for y in range(1, G):
                tok_y(0, y).start()

        @pl.when(c == 1)
        def _():
            for y in range(1, G):
                tok_y(0, y).start()
            for e in range(1, m):
                tok_x(e, 0).start()

        tok_d(q).start()

    def tokens_relay(core):
        @pl.when(c == core)
        def _():
            for k in range(1, Q):
                e, y = k // G, k % G
                if core == 0 and y == 0:
                    tokens_on(nth(k))
                    for far in range(1, G):
                        tok_y(e, far).start()
                if core == 1 and e == 0:
                    tokens_on(nth(k))
                    for far in range(1, m):
                        tok_x(far, y).start()

    def tokens_on(i):
        tok_here(i, c).wait_recv()
        tok_d(i).start()

    def tokens_direct(core):
        @pl.when(c == core)
        def _():
            for k in range(1, Q):
                if (k // G == 0) == (core == 0) and (k // G) * (k % G) == 0:
                    tokens_on(nth(k))

    def tokens_far():
        for k in range(1, Q):
            if (k // G) * (k % G) > 0:
                tokens_on(nth(k))

    def trade_out():
        for j in range(2):
            for a in range(A):
                loop(1, m, lambda e: otrade(j, a, e).start())

    def tokens_sent():
        @pl.when(c == 0)
        def _():
            for e in range(1, m):
                tok_x(e, 0).wait_send()
            for e in range(m):
                for y in range(1, G):
                    tok_y(e, y).wait_send()

        @pl.when(c == 1)
        def _():
            for y in range(1, G):
                tok_y(0, y).wait_send()
            for e in range(1, m):
                for y in range(G):
                    tok_x(e, y).wait_send()

        loop(0, Q, lambda i: tok_d(i).wait_send())

    def halo_kv(i):
        return remote(
            kv.at[i, pl.ds(length, WINDOW)],
            kv.at[i, pl.ds(0, WINDOW)],
            hk_send.at[i],
            hk_recv.at[i],
            {"sp": above},
        )

    def halo_gate(i):
        return remote(
            gate.at[i, pl.ds(length, HALO)],
            gate.at[i, pl.ds(0, HALO)],
            hg_send.at[i],
            hg_recv.at[i],
            {"sp": above},
        )

    def project(j, i):
        block = kvw[...] if j == 0 else wbig[j - 1]
        block = block.reshape(n * m * depth, block.shape[-1])
        return jnp.dot(rows[i], block, preferred_element_type=jnp.float32)

    def do_keys(i):
        tok_here(i, 1 - c).wait_recv()
        kv[i, pl.ds(WINDOW, length), :] = project(0, i).astype(bf16)

        @pl.when(s < n - 1)
        def _():
            halo_kv(i).start()

    def do_query(i):
        query[i] = project(1, i).astype(bf16)

    def do_gate(i):
        gate[i, pl.ds(HALO, length), :] = project(2, i).astype(bf16)

    def do_gated(i):
        values = project(3, i).astype(bf16).astype(jnp.float32)
        here = pl.ds(HALO, length)
        gate[i, here, :] = (gate[i, here, :].astype(jnp.float32) * values).astype(bf16)

        @pl.when(s < n - 1)
        def _():
            halo_gate(i).start()

    def do_conv(i):
        @pl.when(s > 0)
        def _():
            halo_gate(i).wait_recv()

        outer = project(4, i).astype(bf16).astype(jnp.float32)
        gated = gate[i].astype(jnp.float32)
        there = pl.ds(pl.multiple_of(q * slim, LANES), slim)
        mixed = None
        for which in range(TAPS):
            tap = taps[pl.ds(which, 1), there].astype(jnp.float32)
            low = HALO - TAPS + 1 + which
            term = tap * gated[low : low + length]
            mixed = term if mixed is None else mixed + term
        ca[i, :, pl.ds(0, slim)] = (outer * mixed).astype(bf16)

    pairs = 2 * HEAD
    blocks = length // WINDOW
    place_q = lax.broadcasted_iota(jnp.int32, (WINDOW, 2 * WINDOW), 0)
    place_k = lax.broadcasted_iota(jnp.int32, (WINDOW, 2 * WINDOW), 1)
    banded = (place_k > place_q) & (place_k <= place_q + WINDOW)

    def do_attention(i, b):
        row = pl.multiple_of(b * WINDOW, WINDOW)
        band = kv[i, pl.ds(row, 2 * WINDOW), :]
        key, value = band[:, :HEAD], band[:, HEAD:]
        least = jnp.where((s == 0) & (b == 0), WINDOW, 0)
        allowed = banded & (place_k >= least)
        for p in range(heads // 2):
            at = p * pairs
            both = query[i, pl.ds(row, WINDOW), pl.ds(at, pairs)]
            results = []
            for half in range(2):
                one = both[:, half * HEAD : (half + 1) * HEAD]
                scores = lax.dot_general(
                    one, key, (((1,), (1,)), ((), ())), preferred_element_type=jnp.float32
                ) * (1.0 / HEAD**0.5)
                scores = jnp.where(allowed, scores, -jnp.inf)
                logit = sink[q * heads + 2 * p + half]
                peak = jnp.maximum(jnp.max(scores, axis=-1, keepdims=True), logit)
                powers = jnp.exp(scores - peak)
                norm = jnp.sum(powers, axis=-1, keepdims=True) + jnp.exp(logit - peak)
                probs = (powers / norm).astype(bf16)
                results.append(jnp.dot(probs, value, preferred_element_type=jnp.float32))
            ca[i, pl.ds(row, WINDOW), pl.ds(slim + at, pairs)] = jnp.concatenate(
                results, axis=1
            ).astype(bf16)

    def other_plane(d):
        return lax.rem(jnp.where(2 * s >= n, s - d + n, s + d), n)

    def chunks_of(u):
        if U == 1:
            return [(t // m, t % m, 0) for t in range(n * m)]
        if u == 0:
            return [(s, h, a) for h in range(m) for a in range(A)]
        k = min(u, m * A) - 1
        planes = range(1, n)
        if u == m * A:
            planes = range(1, n - 1)
        elif u > m * A:
            planes = range(n - 1, n)
        return [(other_plane(d), k // A, k % A) for d in planes]

    lists = [chunks_of(u) for u in range(U)]
    sizes = [len(chunks) * wa for chunks in lists]
    firsts = [sum(sizes[:u]) for u in range(U)]

    def columns(u):
        return pl.ds(firsts[u], sizes[u])

    def half_rows(half):
        return pl.ds(pl.multiple_of(half * own, LANES), own)

    def core_copy(u, i):
        return remote(
            rows.at[i, half_rows(1 - c), columns(u)],
            precv.at[i, :, columns(u)],
            d_send.at[u, i],
            d_recv.at[u, i],
            other_core,
        )

    def do_out(u, i):
        per = max(1, 2 * LANES // wa)
        for t in range(0, len(lists[u]), per):
            some = lists[u][t : t + per]
            block = jnp.concatenate([w_out[p, h, a] for p, h, a in some], axis=1)
            rows[i, :, pl.ds(firsts[u] + t * wa, len(some) * wa)] = jnp.dot(
                ca[i], block, preferred_element_type=jnp.float32
            ).astype(bf16)
        core_copy(u, i).start()

    counts = ((G, m), (m, G))

    def ordered(v, first, second):
        return seq(second, first) if v == 0 else seq(first, second)

    def to_first(v, e):
        return to_grp(e) if v == 0 else to_fs(e)

    def to_second(v, e):
        return to_fs(e) if v == 0 else to_grp(e)

    def first_copy(u, v, e):
        n2 = counts[v][1]
        which = pl.ds((e - 1) * n2, n2)
        return remote(
            send1.at[v, which, :, columns(u)],
            recv1.at[v, which, :, columns(u)],
            s1_send.at[u, v, e - 1],
            s1_recv.at[u, v, e - 1],
            to_first(v, e),
        )

    def second_copy(u, v, e):
        return remote(
            send2.at[v, e - 1, :, columns(u)],
            recv2.at[v, e - 1, :, columns(u)],
            s2_send.at[u, v, e - 1],
            s2_recv.at[u, v, e - 1],
            to_second(v, e),
        )

    def both_cores(u, v, i):
        at = pl.ds(pl.multiple_of(c * own + v * hr, HALO), hr)
        here = rows[i, at, columns(u)].astype(jnp.float32)
        return here + precv[i, pl.ds(v * hr, hr), columns(u)].astype(jnp.float32)

    def stage_one(u):
        loop(1, Q, lambda k: core_copy(u, nth(k)).wait_recv())
        for v in range(2):
            n1, n2 = counts[v]
            for e in range(1, n1):
                for i2 in range(n2):
                    value = both_cores(u, v, ordered(v, e, i2))
                    send1[v, (e - 1) * n2 + i2, :, columns(u)] = value.astype(bf16)
                first_copy(u, v, e).start()

    def with_first(u, v, i2):
        n1, n2 = counts[v]
        value = both_cores(u, v, ordered(v, 0, i2))
        for e in range(1, n1):
            value = value + recv1[v, (e - 1) * n2 + i2, :, columns(u)].astype(jnp.float32)
        return value

    def stage_two(u):
        for v in range(2):
            n1, n2 = counts[v]
            for e in range(1, n1):
                first_copy(u, v, e).wait_recv()
            for i2 in range(1, n2):
                send2[v, i2 - 1, :, columns(u)] = with_first(u, v, i2).astype(bf16)
                second_copy(u, v, i2).start()

    def stage_three(u):
        core_copy(u, q).wait_recv()
        for v in range(2):
            value = with_first(u, v, 0)
            for i2 in range(1, counts[v][1]):
                second_copy(u, v, i2).wait_recv()
                value = value + recv2[v, i2 - 1, :, columns(u)].astype(jnp.float32)
            value = value.astype(bf16)
            if U == 1:
                out[pl.ds(v * hr, hr), :] = value
            else:
                for k, (p, h, a) in enumerate(lists[u]):
                    at = pl.multiple_of((p * m + h) * across + a * wa, LANES)
                    out[pl.ds(v * hr, hr), pl.ds(at, wa)] = value[:, k * wa : (k + 1) * wa]

    for j in range(5):
        loop(1, m, lambda e: trade(j, e).start())
        if j == 0:
            own_start(0)
    for k in range(m, LEAD, m):
        own_start(k)
    normalize()
    tokens_first()
    for k in range(LEAD):
        if k % m > 0:
            own_start(k)

    @pl.when(s == 0)
    def _():
        kv[:, pl.ds(0, WINDOW), :] = jnp.zeros((Q, WINDOW, 2 * HEAD), bf16)
        gate[:, pl.ds(0, HALO), :] = jnp.zeros((Q, HALO, slim), bf16)

    def attend(unit):
        i = nth(unit // blocks)

        @pl.when((s > 0) & (unit % blocks == 0))
        def _():
            halo_kv(i).wait_recv()

        do_attention(i, unit % blocks)

    span = m * (n - 1)

    def place(base):
        return base * span // 6

    kinds = [0 if k == 0 else 1 if k // G == 0 else 2 if k % G == 0 else 3 for k in range(Q)]
    again = [kinds[:k].count(kinds[k]) for k in range(Q)]

    def times(bases):
        return [(place(bases[kinds[k]]) + again[k], k) for k in range(Q)]

    plan = [
        (do_keys, True, times(KEYS)),
        (do_query, True, times(QUERY)),
        (do_gate, True, times(GATE)),
        (do_gated, True, times(GATED)),
        (
            attend,
            False,
            [
                (place(ATTEND[kinds[k]] + b) + again[k], k * blocks + b)
                for k in range(Q)
                for b in range(blocks)
            ],
        ),
    ]
    relays = [
        (place(RELAY[0]), functools.partial(tokens_relay, 1)),
        (place(RELAY[1]), functools.partial(tokens_direct, 0)),
        (place(RELAY[2]), functools.partial(tokens_relay, 0)),
        (place(RELAY[2]), functools.partial(tokens_direct, 1)),
        (place(RELAY[3]), tokens_far),
        (place(RELAY[2] + 1), trade_out),
    ]

    def tasks(first, count, r):
        for when, run in relays:
            if first <= when < first + count:
                pl.when(r == when - first)(run)
        for run, whole, entries in plan:
            here = [(t - first, k) for t, k in entries if first <= t < first + count]
            if here:
                hit, index = False, 0
                for t, k in here:
                    hit = (r == t) | hit
                    index = jnp.where(r == t, k, index)
                pl.when(hit)(functools.partial(run, nth(index) if whole else index))

    stages = {"o": lambda u: loop(1, Q + 1, lambda r: do_out(u, nth(lax.rem(r, Q))))}
    stages.update({"1": stage_one, "2": stage_two, "3": stage_three})
    def finish(k):
        i = nth(lax.rem(k, Q))
        do_conv(i)
        do_out(0, i)

    last = U - 1
    after = {}
    for u in range(U - 2):
        k, low, high = ins + u, min(1, n - 2), n - 2
        if u > 0:
            after.setdefault((k, 0), []).append(("1", u))
        after.setdefault((k + 1, low), []).append(("2", u))
        after.setdefault((k + 2, low), []).append(("3", u))
        if u < U - 3:
            after.setdefault((k, high), []).append(("o", u + 1))
    ending = (
        [("2", last - 2), ("1", last), ("3", last - 3), ("2", last - 1)]
        + [("3", last - 2), ("2", last), ("3", last - 1), ("3", last)]
        if U > 1
        else [("1", 0), ("2", 0), ("3", 0)]
    )

    for k in range(slots):
        for later in range(LEAD, slots):
            if k == (later - LEAD if later < ins else max(later - OUT_LEAD, ins - LEAD)):
                own_start(later)
        if k == ins and U == 1:
            loop(0, Q, lambda r: do_conv(nth(r)))
            tokens_sent()
        if k >= ins and U > 1:
            for r in range(n - 1):
                if k == ins and r == 0:
                    for later in range(ins, slots):
                        own_ready(later)
                    tokens_sent()
                    loop(1, Q // 2 + 1, finish)
                if k == ins and r == 1:
                    loop(Q // 2 + 1, Q + 1, finish)
                    stages["1"](0)
                arrive(k, r + 1)
                if k == slots - 1 and r == n - 3:
                    stages["o"](last - 1)
                for name, u in after.get((k, r), []):
                    stages[name](u)
                if k == slots - 1 and r == n - 3:
                    stages["1"](last - 1)
                if k == slots - 1 and r == n - 2:
                    stages["o"](last)
            continue

        def body(r):
            arrive(k, r + 1)
            if m <= k < ins:
                tasks((k - m) * (n - 1), n - 1, r)

        loop(0, n - 1, body)
    if U == 1:
        stages["o"](0)
    for name, u in ending:
        stages[name](u)

    for j in range(5):
        loop(1, m, lambda e: trade(j, e).wait_send())
    for j in range(2):
        for a in range(A):
            loop(1, m, lambda e: otrade(j, a, e).wait_send())
    for k in range(slots):
        arrivals_sent(k)

    @pl.when(s < n - 1)
    def _():
        loop(0, Q, lambda i: halo_kv(i).wait_send())
        loop(0, Q, lambda i: halo_gate(i).wait_send())

    for u in range(U):
        loop(0, Q, lambda i: core_copy(u, i).wait_send())
        for v in range(2):
            for e in range(1, counts[v][0]):
                first_copy(u, v, e).wait_send()
            for e in range(1, counts[v][1]):
                second_copy(u, v, e).wait_send()


def local(
    G,
    n,
    m,
    tokens,
    norm_gain,
    w_bgate,
    w_cgate,
    w_conv_in,
    conv_taps,
    w_query,
    w_key,
    w_value,
    sink_logits,
    conv_out_weight,
    attn_out_weight,
):
    own, features = tokens.shape[1:]
    length = 2 * own
    depth, kvwide = w_key.shape
    width = w_query.shape[1]
    across = conv_out_weight.shape[1]
    Q = m * G
    slim = width // Q
    A = 2 if across % (2 * LANES) == 0 else 1
    U = m * A + 2 if across % LANES == 0 else 1
    wa = across // A
    slots = 5 * m + m * A
    n1 = max(m, G) - 1
    cnt = max((G - 1) * m, (m - 1) * G)
    bf16 = jnp.bfloat16
    vmem = pl.BlockSpec(memory_space=pltpu.VMEM)
    dma = pltpu.SemaphoreType.DMA
    mixed = pl.pallas_call(
        functools.partial(kernel, G, n, m, A, U),
        out_shape=jax.ShapeDtypeStruct((own, features), bf16),
        in_specs=[vmem] * 4
        + [pl.BlockSpec(memory_space=pl.ANY)] * 6
        + [vmem, pl.BlockSpec(memory_space=pltpu.SMEM)],
        out_specs=vmem,
        scratch_shapes=[
            pltpu.VMEM((depth, 2 * kvwide), bf16),
            pltpu.VMEM((n, m, depth, 2 * HEAD), bf16),
            pltpu.VMEM((4, n, m, depth, slim), bf16),
            pltpu.VMEM((n, m, A, 2 * slim, wa), bf16),
            pltpu.VMEM((Q, length, features), bf16),
            pltpu.VMEM((Q, WINDOW + length, 2 * HEAD), bf16),
            pltpu.VMEM((Q, length, slim), bf16),
            pltpu.VMEM((Q, HALO + length, slim), bf16),
            pltpu.VMEM((Q, length, 2 * slim), bf16),
            pltpu.VMEM((Q, own, features), bf16),
            pltpu.VMEM((2, cnt, own // 2, features), bf16),
            pltpu.VMEM((2, cnt, own // 2, features), bf16),
            pltpu.VMEM((2, n1, own // 2, features), bf16),
            pltpu.VMEM((2, n1, own // 2, features), bf16),
            dma((5,)),
            dma((2, A)),
            dma((5, m)),
            dma((5, m)),
            dma((2, A, m)),
            dma((2, A, m)),
            dma((slots, 2, n)),
            dma((slots, n)),
            dma((m, G)),
            dma((m, G)),
            dma((Q,)),
            dma((Q, 2)),
            dma((Q,)),
            dma((Q,)),
            dma((Q,)),
            dma((Q,)),
            dma((U, Q)),
            dma((U, Q)),
            dma((U, 2, n1)),
            dma((U, 2, n1)),
            dma((U, 2, n1)),
            dma((U, 2, n1)),
        ],
        compiler_params=pltpu.CompilerParams(
            collective_id=0, has_side_effects=True, vmem_limit_bytes=67_000_000
        ),
    )(
        tokens[0],
        norm_gain[None],
        w_key,
        w_value,
        w_query,
        w_cgate,
        w_conv_in,
        w_bgate,
        conv_out_weight,
        attn_out_weight,
        conv_taps,
        sink_logits,
    )
    return mixed[None]


def solution(mesh):
    placed = (
        P(("grp", "fs"), ("sp", "tp"), None),
        P(),
        P(("sp", "fs"), "tp"),
        P(("sp", "fs"), "tp"),
        P(("sp", "fs"), "tp"),
        P(None, "tp"),
        P(("sp", "fs"), "tp"),
        P(("sp", "fs"), "tp"),
        P(("sp", "fs"), "tp"),
        P("tp"),
        P("tp", ("sp", "fs")),
        P("tp", ("sp", "fs")),
    )
    return jax.shard_map(
        functools.partial(local, mesh.shape["grp"], mesh.shape["sp"], mesh.shape["fs"]),
        mesh=mesh,
        in_specs=placed,
        out_specs=P(("grp", "fs"), ("sp", "tp"), None),
        check_vma=False,
    )
```
